32 devices in a mesh: grp: 2 (over y), ep: 8 (over z, x), tp: 2 (over core).
Axes of the slice: x: 2, y: 2, z: 4, core: 2. Of those that a mesh axis runs over, the one named last changes fastest.
Arguments:
- fresh_inputs: bfloat16 [256, 2048], P(('grp', 'ep')), parts along dimension 0, may hold values from -6 to 6
- memory_arrays: float32 [256, 32, 64, 64], P(('grp', 'ep'), 'tp'), parts along dimension 0, may hold values from -4 to 4
- chosen_specialist: int32 [256, 2], P(('grp', 'ep')), parts along dimension 0, may hold values from 0 to 3, all different within a row; in each aligned block of 128 rows (0 to 127, 128 to 255, ...) at most 96 rows name the same one
- chosen_coefficient: bfloat16 [256, 2], P(('grp', 'ep')), parts along dimension 0, may hold values from 0.25 to 1
- first_rescale: float32 [2048], replicated, may hold values from 0.1 to 1.9
- second_rescale: float32 [2048], replicated, may hold values from 0.1 to 1.9
- receiver_projector: bfloat16 [2048, 2048], P('tp', 'ep'), may hold values from -0.125 to 0.125
- address_projector: bfloat16 [2048, 2048], P('tp', 'ep'), may hold values from -0.125 to 0.125
- content_projector: bfloat16 [2048, 2048], P('tp', 'ep'), may hold values from -0.125 to 0.125
- final_projector: bfloat16 [2048, 2048], P('tp', 'ep'), may hold values from -0.125 to 0.125
- forget_narrowing: bfloat16 [2048, 64], replicated, may hold values from -0.125 to 0.125
- forget_widening: bfloat16 [64, 2048], P(None, 'tp'), may hold values from -0.75 to 0.75
- forget_bias: float32 [2048], P('tp'), may hold values from -3 to 1
- learning_narrowing: bfloat16 [2048, 64], replicated, may hold values from -0.125 to 0.125
- learning_widening: bfloat16 [64, 2048], P(None, 'tp'), may hold values from -0.75 to 0.75
- learning_bias: float32 [2048], P('tp'), may hold values from -1.5 to 1.5
- lane_scaling: float32 [2048], P('tp'), may hold values from 0.1 to 1.9
- instant_reward: float32 [32, 64], P('tp'), may hold values from -0.5 to 0.5
- specialist_switch: bfloat16 [2048, 28672], P(None, ('ep', 'tp')), may hold values from -0.125 to 0.125
- specialist_expand: bfloat16 [2048, 28672], P(None, ('ep', 'tp')), may hold values from -0.125 to 0.125
- specialist_contract: bfloat16 [28672, 2048], P(('ep', 'tp')), may hold values from -0.0625 to 0.0625
- common_activator: bfloat16 [2048, 5632], P(None, ('ep', 'tp')), may hold values from -0.125 to 0.125
- common_expand: bfloat16 [2048, 5632], P(None, ('ep', 'tp')), may hold values from -0.125 to 0.125
- common_contract: bfloat16 [5632, 2048], P(('ep', 'tp')), may hold values from -0.078125 to 0.078125
- common_switch: bfloat16 [2048], replicated, may hold values from -0.125 to 0.125
Outputs:
- new_tokens: bfloat16 [256, 2048], P(('grp', 'ep', 'tp')), parts along dimension 0
- memory_after: float32 [256, 32, 64, 64], P(('grp', 'ep'), 'tp'), parts along dimension 0
The draws below stay inside these ranges and needn't reach their ends.
There are 2 independent parts, one for each index of `grp`. The reference program is written for one: setup_inputs(seed, part) draws one part's arguments, and reference() takes and returns one part's arrays. A program takes and returns all parts, laid end to end along the dimension named above; an argument that names none is the same for every part. Nothing has to cross between parts.
Inputs may be any that keep to these rules, and one draw needn't show every extreme that they name: `chosen_specialist`: each row names 2 different experts. Over the whole batch no expert is named by more than 96 rows, and in every draw some expert is named by exactly 96 rows.
All inputs are finite; a program needn't handle non-finite values.
Results may differ from the reference program's by a relative error of at most 0.014.
Values may be sent and summed in bfloat16 or wider, within the bound.
A program may use at most 128 MiB of HBM per device.

```python
import math
import jax
import jax.numpy as jnp
import numpy as np
from jax import lax

MODEL_DIM = 2048
LANE_WIDTH = 64
LANE_COUNT = 32
LOWRANK_DIM = 64
EXPERTS = 4
TOP_K = 2
FF_E = 7168
DENSE_FF = 5632
BATCH = 128
CAP = 96
N_TP = 2


def block_levels(rng, shape, pieces, low, largest):
    level, own = 1.0, jax.random.fold_in(rng, 6)
    for dim, parts in pieces:
        steps = jnp.exp(jax.random.uniform(jax.random.fold_in(own, dim), (parts,), jnp.float32, low / len(pieces), largest / len(pieces)))
        level = level * jnp.repeat(steps, shape[dim] // parts).reshape([-1 if axis == dim else 1 for axis in range(len(shape))])
    return level


def assign_block(stream_key, own, number, rows, amount, top, most, lean):
    ranking = jax.random.permutation(stream_key, amount)
    packed, common = shares(amount, rows * top, most, lean, True), shares(amount, rows * top, most, lean, False)
    places = jnp.arange(amount)

    def named(tallies, offset_by):
        used = int((tallies > 0).sum())
        fixed = max(1, used // 4)
        moved = fixed + (places - fixed + offset_by * (used - fixed)) % max(1, amount - fixed)
        return jnp.zeros((amount,), jnp.int32).at[ranking[jnp.where(places < fixed, places, moved)]].set(jnp.asarray(tallies, jnp.int32))

    tallies = jnp.where(number % 4 == 0, named(packed, number // 4), named(common, number - number // 4 - 1))
    mixed = jax.random.permutation(jax.random.fold_in(own, 3), amount)
    source_of, sink = mixed[0:amount // 2 * 2:2], mixed[1:amount // 2 * 2:2]
    slack = jnp.minimum(tallies[source_of] - 1, most - tallies[sink]) // 2
    slack = jnp.where((source_of == ranking[0]) | (sink == ranking[0]) | (tallies[sink] == 0), 0, jnp.maximum(slack, 0))
    moved = jax.random.randint(jax.random.fold_in(own, 4), (amount // 2,), 0, 1 << 20) % (slack + 1)
    tallies = tallies.at[source_of].add(-moved).at[sink].add(moved)
    members = jnp.searchsorted(jnp.cumsum(tallies), jnp.arange(rows * top), side="right").astype(jnp.int32)
    listing = members.reshape(top, rows).T
    listing = listing[jax.random.permutation(jax.random.fold_in(own, 1), rows)]
    offset_by = jax.random.randint(jax.random.fold_in(own, 2), (rows, 1), 0, top)
    return jnp.take_along_axis(listing, (jnp.arange(top)[None, :] + offset_by) % top, axis=1)


def shares(count, total, reach, lean, full):
    portions = [(1 << 20) // math.isqrt(rank ** lean) + 1 for rank in range(1, count + 1)]
    largest = reach if full else min(reach, max(-(-total // count), total * portions[0] // sum(portions)))
    least = 1 if total - largest >= count - 1 else 0
    holding, surplus = [largest] + [least] * (count - 1), total - largest - least * (count - 1)
    while surplus > 0:
        free = [i for i in range(1, count) if holding[i] < largest] or [i for i in range(1, count) if holding[i] < reach]
        pool, remaining = sum([portions[i] for i in free]), surplus
        for i in free:
            addition = min(reach - holding[i], max(1, remaining * portions[i] // pool), surplus)
            holding[i] = holding[i] + addition
            surplus = surplus - addition
    return np.array(holding)


def bell_draw(rng, dims, deviation, limit, cuts=(), dtype=jnp.bfloat16):
    gain = block_levels(rng, dims, cuts, -0.22, 0.18) if cuts else 1.0
    drawn = jax.random.normal(rng, dims, jnp.float32) * deviation * gain
    return jnp.minimum(jnp.maximum(drawn, -limit), limit).astype(dtype)


def setup_inputs(seed: int = 0, part: int = 0) -> dict:
    splits = jax.random.split(jax.random.key(seed), 26)
    own_keys = jax.random.split(jax.random.fold_in(splits[25], part), 26)
    fresh_inputs = bell_draw(own_keys[0], (BATCH, MODEL_DIM), 1.0, 6.0, ((0, 8),))
    memory_arrays = bell_draw(own_keys[1], (BATCH, LANE_COUNT, LANE_WIDTH, LANE_WIDTH), 0.5, 4.0, ((0, 8), (1, 2)), jnp.float32)
    chosen_specialist_keys = jax.random.split(jax.random.fold_in(own_keys[2], 1), BATCH // BATCH)
    chosen_specialist_turns = jax.random.permutation(jax.random.fold_in(own_keys[2], 3), BATCH // BATCH)
    chosen_specialist = jax.vmap(lambda own, number: assign_block(jax.random.fold_in(own_keys[2], 2), own, number, BATCH, EXPERTS, TOP_K, CAP, 2))(chosen_specialist_keys, chosen_specialist_turns).reshape((BATCH, TOP_K))
    chosen_coefficient = jnp.clip(0.25 + 0.75 * jax.random.uniform(own_keys[3], (BATCH, TOP_K), jnp.float32) ** block_levels(own_keys[3], (BATCH, TOP_K), ((0, 8),), -0.2, 0.2), 0.25, 1.0).astype(jnp.bfloat16)
    first_rescale = jnp.clip(1.0 + 0.18 * jax.random.normal(splits[4], (MODEL_DIM,), jnp.float32), 0.1, 1.9)
    second_rescale = jnp.clip(1.0 + 0.18 * jax.random.normal(splits[5], (MODEL_DIM,), jnp.float32), 0.1, 1.9)
    receiver_projector = bell_draw(splits[6], (MODEL_DIM, MODEL_DIM), MODEL_DIM ** -0.5, 0.125, ((0, 2), (1, 8)))
    address_projector = bell_draw(splits[7], (MODEL_DIM, MODEL_DIM), MODEL_DIM ** -0.5, 0.125, ((0, 2), (1, 8)))
    content_projector = bell_draw(splits[8], (MODEL_DIM, MODEL_DIM), MODEL_DIM ** -0.5, 0.125, ((0, 2), (1, 8)))
    final_projector = bell_draw(splits[9], (MODEL_DIM, MODEL_DIM), MODEL_DIM ** -0.5, 0.125, ((0, 2), (1, 8)))
    forget_narrowing = bell_draw(splits[10], (MODEL_DIM, LOWRANK_DIM), MODEL_DIM ** -0.5, 0.125)
    forget_widening = bell_draw(splits[11], (LOWRANK_DIM, MODEL_DIM), LOWRANK_DIM ** -0.5, 0.75, ((1, 2),))
    forget_bias = jnp.clip(-3.0 + 4.0 * jax.random.uniform(splits[12], (MODEL_DIM,), jnp.float32) ** block_levels(splits[12], (MODEL_DIM,), ((0, 2),), -0.2, 0.2), -3.0, 1.0)
    learning_narrowing = bell_draw(splits[13], (MODEL_DIM, LOWRANK_DIM), MODEL_DIM ** -0.5, 0.125)
    learning_widening = bell_draw(splits[14], (LOWRANK_DIM, MODEL_DIM), LOWRANK_DIM ** -0.5, 0.75, ((1, 2),))
    learning_bias = jnp.clip(jax.random.uniform(splits[15], (MODEL_DIM,), jnp.float32, -1.5, 1.5) * block_levels(splits[15], (MODEL_DIM,), ((0, 2),), -0.4, 0.0), -1.5, 1.5)
    lane_scaling = jnp.clip(1.0 + 0.18 * jax.random.normal(splits[16], (MODEL_DIM,), jnp.float32), 0.1, 1.9)
    instant_reward = bell_draw(splits[17], (LANE_COUNT, LANE_WIDTH), 0.1, 0.5, ((0, 2),), jnp.float32)
    specialist_switch = bell_draw(splits[18], (MODEL_DIM, EXPERTS * FF_E), MODEL_DIM ** -0.5, 0.125, ((1, 16),))
    specialist_expand = bell_draw(splits[19], (MODEL_DIM, EXPERTS * FF_E), MODEL_DIM ** -0.5, 0.125, ((1, 16),))
    specialist_contract = bell_draw(splits[20], (EXPERTS * FF_E, MODEL_DIM), FF_E ** -0.5, 0.0625, ((0, 16),))
    common_activator = bell_draw(splits[21], (MODEL_DIM, DENSE_FF), MODEL_DIM ** -0.5, 0.125, ((1, 16),))
    common_expand = bell_draw(splits[22], (MODEL_DIM, DENSE_FF), MODEL_DIM ** -0.5, 0.125, ((1, 16),))
    common_contract = bell_draw(splits[23], (DENSE_FF, MODEL_DIM), DENSE_FF ** -0.5, 0.078125, ((0, 16),))
    common_switch = bell_draw(splits[24], (MODEL_DIM,), MODEL_DIM ** -0.5, 0.125)
    return dict(fresh_inputs=fresh_inputs, memory_arrays=memory_arrays, chosen_specialist=chosen_specialist, chosen_coefficient=chosen_coefficient, first_rescale=first_rescale, second_rescale=second_rescale, receiver_projector=receiver_projector, address_projector=address_projector, content_projector=content_projector, final_projector=final_projector, forget_narrowing=forget_narrowing, forget_widening=forget_widening, forget_bias=forget_bias, learning_narrowing=learning_narrowing, learning_widening=learning_widening, learning_bias=learning_bias, lane_scaling=lane_scaling, instant_reward=instant_reward, specialist_switch=specialist_switch, specialist_expand=specialist_expand, specialist_contract=specialist_contract, common_activator=common_activator, common_expand=common_expand, common_contract=common_contract, common_switch=common_switch)


RMS_EPS = 1e-06
GROUP_EPS = 0.00064
HIGHEST = lax.Precision.HIGHEST

def rms_norm(values, norm_gain):
    mean_sq = lax.optimization_barrier(jnp.mean(values * values, axis=-1, keepdims=True))
    return values * lax.rsqrt(mean_sq + RMS_EPS) * norm_gain

def split_product(left_rows, weight_rows):
    block_width = left_rows.shape[1] // N_TP
    running = jnp.zeros((left_rows.shape[0], weight_rows.shape[1]), jnp.float32)
    for block_index in range(N_TP):
        lower = block_index * block_width
        product = jnp.dot(left_rows[:, lower:lower + block_width], weight_rows[lower:lower + block_width], preferred_element_type=jnp.float32)
        running = running + lax.optimization_barrier(product.astype(jnp.bfloat16)).astype(jnp.float32)
    return running.astype(jnp.bfloat16)

def evolve_memory(memory_arrays, receiver_lanes, address_lanes, content_lanes, forget_lanes, learning_lanes, lane_rescale, instant_reward):
    unit_key = address_lanes * lax.rsqrt(lax.optimization_barrier(jnp.sum(address_lanes * address_lanes, axis=-1, keepdims=True)) + 1.0)
    stepped_address = address_lanes * learning_lanes
    removal = jnp.einsum('bhvk,bhk->bhv', memory_arrays, unit_key, precision=HIGHEST)
    memory_after = memory_arrays * forget_lanes[:, :, None, :] - removal[..., None] * (unit_key * learning_lanes)[:, :, None, :] + content_lanes[..., None] * stepped_address[:, :, None, :]
    memory_retrieval = jnp.einsum('bhvk,bhk->bhv', memory_after, receiver_lanes, precision=HIGHEST)
    centred = memory_retrieval - lax.optimization_barrier(jnp.mean(memory_retrieval, axis=-1, keepdims=True))
    unit_address = centred * lax.rsqrt(lax.optimization_barrier(jnp.mean(centred * centred, axis=-1, keepdims=True)) + GROUP_EPS)
    instant_extra = lax.optimization_barrier(jnp.sum(receiver_lanes * stepped_address * instant_reward, axis=-1, keepdims=True)) * content_lanes
    return (memory_after, unit_address * lane_rescale + instant_extra)

def swiglu(rows_in, gate_w, up_w):
    gate_val = jnp.dot(rows_in, gate_w, preferred_element_type=jnp.float32)
    up_val = jnp.dot(rows_in, up_w, preferred_element_type=jnp.float32)
    return (jax.nn.silu(gate_val) * up_val).astype(jnp.bfloat16)

def reference(fresh_inputs, memory_arrays, chosen_specialist, chosen_coefficient, first_rescale, second_rescale, receiver_projector, address_projector, content_projector, final_projector, forget_narrowing, forget_widening, forget_bias, learning_narrowing, learning_widening, learning_bias, lane_scaling, instant_reward, specialist_switch, specialist_expand, specialist_contract, common_activator, common_expand, common_contract, common_switch):
    batch_rows = fresh_inputs.shape[0]
    residual = fresh_inputs.astype(jnp.float32)
    normed = rms_norm(residual, first_rescale).astype(jnp.bfloat16)
    receiver_array = split_product(normed, receiver_projector)
    address_mapped = split_product(normed, address_projector)
    content_array = split_product(normed, content_projector)
    decay_mid = jnp.tanh(jnp.dot(normed, forget_narrowing, preferred_element_type=jnp.float32)).astype(jnp.bfloat16)
    decay_pre = forget_bias + jnp.dot(decay_mid, forget_widening, preferred_element_type=jnp.float32)
    forget_multiplier = jnp.exp(-jnp.exp(-jax.nn.softplus(-decay_pre) - 0.5))
    rate_mid = jnp.dot(normed, learning_narrowing, preferred_element_type=jnp.float32).astype(jnp.bfloat16)
    learning_step = jax.nn.sigmoid(learning_bias + jnp.dot(rate_mid, learning_widening, preferred_element_type=jnp.float32))

    def divide_lanes(channels):
        return channels.astype(jnp.float32).reshape(batch_rows, LANE_COUNT, LANE_WIDTH)
    memory_after, memory_retrieval = evolve_memory(memory_arrays, divide_lanes(receiver_array), divide_lanes(address_mapped), divide_lanes(content_array), divide_lanes(forget_multiplier), divide_lanes(learning_step), lane_scaling.reshape(LANE_COUNT, LANE_WIDTH), instant_reward)
    attended = memory_retrieval.reshape(batch_rows, MODEL_DIM).astype(jnp.bfloat16)
    mixed = split_product(attended, final_projector)
    residual = residual + mixed.astype(jnp.float32)
    ffn_in = rms_norm(residual, second_rescale).astype(jnp.bfloat16)
    routed = jnp.zeros((batch_rows, MODEL_DIM), jnp.float32)
    for expert in range(EXPERTS):
        lower = expert * FF_E
        hidden = swiglu(ffn_in, specialist_switch[:, lower:lower + FF_E], specialist_expand[:, lower:lower + FF_E])
        share = lax.optimization_barrier(jnp.sum(jnp.where(chosen_specialist == expert, chosen_coefficient.astype(jnp.float32), 0.0), axis=1))
        routed = routed + share[:, None] * jnp.dot(hidden, specialist_contract[lower:lower + FF_E], preferred_element_type=jnp.float32)
    shared_hidden = swiglu(ffn_in, common_activator, common_expand)
    branch_scale = jax.nn.sigmoid(jnp.dot(ffn_in, common_switch, preferred_element_type=jnp.float32))
    routed = routed + branch_scale[:, None] * jnp.dot(shared_hidden, common_contract, preferred_element_type=jnp.float32)
    return ((residual + routed).astype(jnp.bfloat16), memory_after)
```

```python
import functools
import math

import jax
import jax.numpy as jnp
from jax import lax
from jax.experimental import pallas as pl
from jax.experimental.pallas import tpu as pltpu
from jax.sharding import PartitionSpec as P

LANE_WIDTH = 64
FF_E = 7168


RMS_EPS = 1e-06
GROUP_EPS = 0.00064
HIGHEST = lax.Precision.HIGHEST
MESH = pl.DeviceIdType.MESH
VMEM_ROOM = 52 * 2**20


def rms_norm(values, norm_gain):
    mean_sq = jnp.mean(values * values, axis=-1, keepdims=True)
    return values * lax.rsqrt(mean_sq + RMS_EPS) * norm_gain


def widen(rounded):
    return lax.optimization_barrier(rounded).astype(jnp.float32)


def evolve_memory(
    memory_arrays,
    receiver_lanes,
    address_lanes,
    content_lanes,
    forget_lanes,
    learning_lanes,
    lane_rescale,
    instant_reward,
):
    unit_key = address_lanes * lax.rsqrt(
        jnp.sum(address_lanes * address_lanes, axis=-1, keepdims=True) + 1.0
    )
    stepped_address = address_lanes * learning_lanes
    removal = jnp.einsum("bhvk,bhk->bhv", memory_arrays, unit_key, precision=HIGHEST)
    memory_after = (
        memory_arrays * forget_lanes[:, :, None, :]
        - removal[..., None] * (unit_key * learning_lanes)[:, :, None, :]
        + content_lanes[..., None] * stepped_address[:, :, None, :]
    )
    memory_retrieval = jnp.einsum("bhvk,bhk->bhv", memory_after, receiver_lanes, precision=HIGHEST)
    centred = memory_retrieval - jnp.mean(memory_retrieval, axis=-1, keepdims=True)
    unit_address = centred * lax.rsqrt(
        jnp.mean(centred * centred, axis=-1, keepdims=True) + GROUP_EPS
    )
    instant_extra = (
        jnp.sum(receiver_lanes * stepped_address * instant_reward, axis=-1, keepdims=True)
        * content_lanes
    )
    return (memory_after, unit_address * lane_rescale + instant_extra)


def swiglu(rows_in, gate_w, up_w):
    gate_val = jnp.dot(rows_in, gate_w, preferred_element_type=jnp.float32)
    up_val = jnp.dot(rows_in, up_w, preferred_element_type=jnp.float32)
    return (jax.nn.silu(gate_val) * up_val).astype(jnp.bfloat16)


def body(
    fresh_inputs,
    memory_arrays,
    chosen_specialist,
    chosen_coefficient,
    first_rescale,
    second_rescale,
    receiver_projector,
    address_projector,
    content_projector,
    final_projector,
    forget_narrowing,
    forget_widening,
    forget_bias,
    learning_narrowing,
    learning_widening,
    learning_bias,
    lane_scaling,
    instant_reward,
    specialist_switch,
    specialist_expand,
    specialist_contract,
    common_activator,
    common_expand,
    common_contract,
    common_switch,
):
    own_rows = fresh_inputs.shape[0]
    model_width = fresh_inputs.shape[1]
    tp_count = lax.axis_size("tp")
    tp_rank = lax.axis_index("tp")
    half_width = model_width // tp_count
    head_count = half_width // LANE_WIDTH
    residual = fresh_inputs.astype(jnp.float32)
    normed = rms_norm(residual, first_rescale).astype(jnp.bfloat16)
    normed_half = lax.dynamic_slice_in_dim(normed, tp_rank * half_width, half_width, 1)
    local_weights = jnp.stack((receiver_projector, address_projector, content_projector), axis=1)
    projected_rows = jnp.einsum(
        "rd,dkc->rkc",
        lax.all_gather(normed_half, "ep", axis=0, tiled=True),
        local_weights,
        preferred_element_type=jnp.float32,
    ).astype(jnp.bfloat16)
    partial_value = lax.all_to_all(projected_rows, "ep", split_axis=0, concat_axis=2, tiled=True)
    projected = lax.psum(widen(partial_value).astype(jnp.bfloat16), "tp")
    mine = lax.dynamic_slice_in_dim(projected, tp_rank * half_width, half_width, 2)

    def divide_lanes(channels):
        return channels.astype(jnp.float32).reshape(own_rows, head_count, LANE_WIDTH)

    decay_mid = jnp.tanh(
        jnp.dot(normed, forget_narrowing, preferred_element_type=jnp.float32)
    ).astype(jnp.bfloat16)
    decay_pre = forget_bias + jnp.dot(
        decay_mid, forget_widening, preferred_element_type=jnp.float32
    )
    decay_vals = jnp.exp(-jnp.exp(-jax.nn.softplus(-decay_pre) - 0.5))
    rate_mid = jnp.dot(normed, learning_narrowing, preferred_element_type=jnp.float32).astype(
        jnp.bfloat16
    )
    rate_vals = jax.nn.sigmoid(
        learning_bias + jnp.dot(rate_mid, learning_widening, preferred_element_type=jnp.float32)
    )
    memory_after, memory_retrieval = evolve_memory(
        memory_arrays,
        divide_lanes(mine[:, 0]),
        divide_lanes(mine[:, 1]),
        divide_lanes(mine[:, 2]),
        divide_lanes(decay_vals),
        divide_lanes(rate_vals),
        lane_scaling.reshape(head_count, LANE_WIDTH),
        instant_reward,
    )
    attended = memory_retrieval.reshape(own_rows, half_width).astype(jnp.bfloat16)
    done_rows = jnp.dot(
        lax.all_gather(attended, "ep", axis=0, tiled=True),
        final_projector,
        preferred_element_type=jnp.float32,
    ).astype(jnp.bfloat16)
    out_part = lax.all_to_all(done_rows, "ep", split_axis=0, concat_axis=1, tiled=True)
    mixed_out = lax.psum(widen(out_part).astype(jnp.bfloat16), "tp")
    residual = residual + mixed_out.astype(jnp.float32)
    ffn_in = rms_norm(residual, second_rescale).astype(jnp.bfloat16)
    all_in, all_weight, all_ids = (
        lax.all_gather(ffn_in, "ep", axis=0, tiled=True),
        lax.all_gather(chosen_coefficient, "ep", axis=0, tiled=True),
        lax.all_gather(chosen_specialist, "ep", axis=0, tiled=True),
    )
    column_count = specialist_switch.shape[1]
    flat_rank = lax.axis_index("ep") * tp_count + tp_rank
    expert = flat_rank * column_count // FF_E
    expert_share = jnp.sum(
        jnp.where(all_ids == expert, all_weight.astype(jnp.float32), 0.0), axis=1
    )
    hidden = swiglu(all_in, specialist_switch, specialist_expand)
    shared_hidden = swiglu(all_in, common_activator, common_expand)
    branch_scale = jax.nn.sigmoid(
        jnp.dot(all_in, common_switch, preferred_element_type=jnp.float32)
    )
    rows_mine = own_rows // tp_count
    expert_term = expert_share[:, None] * jnp.dot(
        hidden, specialist_contract, preferred_element_type=jnp.float32
    )
    routed = lax.psum_scatter(
        expert_term
        + branch_scale[:, None]
        * jnp.dot(shared_hidden, common_contract, preferred_element_type=jnp.float32),
        ("ep", "tp"),
        scatter_dimension=0,
        tiled=True,
    )
    own_residual = lax.dynamic_slice_in_dim(residual, tp_rank * rows_mine, rows_mine, 0)
    return ((own_residual + routed).astype(jnp.bfloat16), memory_after)


def flipped(index, mask):
    for bit in range(mask.bit_length()):
        step = 1 << bit
        if mask & step:
            index = index + step * (1 - 2 * lax.rem(index // step, 2))
    return index


def _greet(ep, tp):
    me, core = lax.axis_index("ep"), lax.axis_index("tp")
    barrier = pltpu.get_barrier_semaphore()
    for mask in range(ep - 1, -1, -1):
        for side in range(tp):
            if mask or side:
                pl.semaphore_signal(
                    barrier,
                    inc=1,
                    device_id={"ep": flipped(me, mask), "tp": lax.rem(core + side, tp)},
                    device_id_type=MESH,
                )


def _met(ep, tp):
    pl.semaphore_wait(pltpu.get_barrier_semaphore(), ep * tp - 1)


def _remote(src, dst, send, recv, e, t):
    return pltpu.make_async_remote_copy(
        src_ref=src,
        dst_ref=dst,
        send_sem=send,
        recv_sem=recv,
        device_id={"ep": e, "tp": t},
        device_id_type=MESH,
    )


def across_dot(left, right):
    return lax.dot_general(
        left, right, (((1,), (1,)), ((), ())), preferred_element_type=jnp.float32
    )


def by_head(ref, channels, first):
    for h in range(channels.shape[1] // LANE_WIDTH):
        ref[:, first + h, :] = channels[:, h * LANE_WIDTH : (h + 1) * LANE_WIDTH]


def arrive(ref, sem):
    pltpu.make_async_copy(ref, ref, sem).wait()


def layer_kernel(
    ep, tp, expert_cols,
    x_h, memory, ids_h, coef_h, gain_h, gain2_h, cs_h, reward_h, scaling_h,
    wq_h, wk_h, wv_h, wo_h, fnar_h, fwid_h, fbias_h, lnar_h, lwid_h, lbias_h,
    wg_h, wu_h, wd_h, cg_h, cu_h, cd_h,
    out, mem,
    x, ids, coef, gain, gain2, cs, reward, scaling, fnar, fwid, fbias, lnar, lwid, lbias,
    w, wo, wg, wu, wd, cg, cu, cd, pk, pk16,
    halves, rows_all, part, gotp, query, key, value, decay, rate, dch, lane_gain,
    flip, probes, moves, factors, read,
    att, att_all, xcol, share, pbuf, psib, res, ffn, hid, chid, sibout, sibin, mine, got,
    lsem, msem, wsem,
    s_row, r_row, s_part, r_part, s_att, r_att, s_x, r_x, s_sh, r_sh, s_p, r_p,
    s_res, r_res, f_res, b_res, s_sib, r_sib, s_out, r_out,
):
    me, core = lax.axis_index("ep"), lax.axis_index("tp")
    mate = lax.rem(core + 1, tp)
    group = ep // tp
    side = me // group
    own, width = x.shape
    half = width // tp
    cols = wo.shape[1]
    rows = ep * own
    heads = lane_gain.shape[0]
    pack = pk.shape[2] // LANE_WIDTH
    packs = heads // pack
    block_rows = packs * LANE_WIDTH
    far = list(range(ep - 1, 0, -1))
    _greet(ep, tp)

    smalls = [
        pltpu.make_async_copy(a, b, lsem.at[i])
        for i, (a, b) in enumerate(
            (
                (x_h, x), (gain_h, gain), (fnar_h, fnar), (fwid_h, fwid), (fbias_h, fbias),
                (lnar_h, lnar), (lwid_h, lwid), (lbias_h, lbias), (scaling_h, scaling),
                (reward_h, reward), (ids_h, ids), (coef_h, coef), (gain2_h, gain2), (cs_h, cs),
            )
        )
    ]
    weights = [
        pltpu.make_async_copy(a, b, wsem.at[i])
        for i, (a, b) in enumerate(
            (
                (wq_h, w.at[0]), (wk_h, w.at[1]), (wv_h, w.at[2]), (wo_h, wo), (wg_h, wg),
                (wu_h, wu), (cg_h, cg), (cu_h, cu), (wd_h, wd), (cd_h, cd),
            )
        )
    ]
    batches = msem.shape[0]
    batch = own // batches
    states = [
        pltpu.make_async_copy(
            memory.at[pl.ds(i * batch, batch)], mem.at[pl.ds(i * batch, batch)], msem.at[i]
        )
        for i in range(batches)
    ]
    for copy in smalls + weights[:3] + states:
        copy.start()
    sends = []

    def push(*args):
        sends.append(_remote(*args))
        sends[-1].start()

    for copy in smalls[:2]:
        copy.wait()
    normed = rms_norm(x[...].astype(jnp.float32), gain[...]).astype(jnp.bfloat16)
    for i in range(tp):
        halves[i] = normed[:, i * half : (i + 1) * half]
    _met(ep, tp)
    for k in far:
        push(halves.at[core], rows_all.at[me], s_row.at[k], r_row.at[me], flipped(me, k), core)
    rows_all[me] = halves[core]

    for copy in smalls[2:]:
        copy.wait()
    decay_mid = jnp.tanh(across_dot(normed, fnar[...])).astype(jnp.bfloat16)
    decay_pre = fbias[...] + jnp.dot(decay_mid, fwid[...], preferred_element_type=jnp.float32)
    kept = jnp.exp(-(math.exp(-0.5) / (1.0 + jnp.exp(-decay_pre))))
    dch[...] = kept
    by_head(decay, kept, 0)
    rate_mid = across_dot(normed, lnar[...]).astype(jnp.bfloat16)
    rate_pre = lbias[...] + jnp.dot(rate_mid, lwid[...], preferred_element_type=jnp.float32)
    by_head(rate, 1.0 / (1.0 + jnp.exp(-rate_pre)), 0)
    for h in range(heads):
        lane_gain[h : h + 1] = scaling[:, h * LANE_WIDTH : (h + 1) * LANE_WIDTH]
    for ref in (flip, probes, moves):
        ref[...] = jnp.zeros_like(ref)
    lane = lax.broadcasted_iota(jnp.int32, (own, 128), 1)
    routes = jnp.zeros((own, 128), jnp.float32)
    ids_cols, coef_cols = ids[...].T, coef[...].astype(jnp.float32).T
    for i in range(ids.shape[0]):
        routes = routes + jnp.where(
            ids_cols[:, i : i + 1] == lane, coef_cols[:, i : i + 1], 0.0
        )
    share[me] = routes.astype(jnp.bfloat16)
    xcol[me] = x[:, pl.ds(pl.multiple_of(me * cols, cols), cols)]
    for copy in states:
        copy.wait()
    for copy in weights[3:]:
        copy.start()

    def join(b, _):
        for p in range(packs):
            joined = jnp.concatenate([mem[b, p * pack + i] for i in range(pack)], axis=-1)
            at = slice(p * LANE_WIDTH, (p + 1) * LANE_WIDTH)
            pk[b, at] = joined
            pk16[b, at] = joined.astype(jnp.bfloat16)
        return _

    lax.fori_loop(0, own, join, 0)

    for copy in weights[:3]:
        copy.wait()
    for k in far:
        e = flipped(me, k)
        arrive(rows_all.at[e], r_row.at[e])
    every = rows_all[...].reshape(rows, half)
    for i in range(3):
        done = jnp.dot(every, w[i], preferred_element_type=jnp.float32)
        part[:, i] = done.astype(jnp.bfloat16).reshape(ep, own, cols)
    slot = core * group + lax.rem(me, group)
    for k in far:
        e = flipped(me, k)
        push(part.at[e], gotp.at[slot], s_part.at[k], r_part.at[slot], e, side)
    here = side == core
    local = pltpu.make_async_copy(part.at[me], gotp.at[slot], r_part.at[slot])
    across = _remote(part.at[me], gotp.at[slot], s_part.at[0], r_part.at[slot], me, side)

    @pl.when(here)
    def _():
        local.start()

    @pl.when(jnp.logical_not(here))
    def _():
        across.start()

    blocks = []
    for k in far:
        e = flipped(me, k)
        block = x.at[:, pl.ds(pl.multiple_of(e * cols, cols), cols)]
        blocks.append(_remote(block, xcol.at[me], s_x.at[k], r_x.at[me], e, core))

    @pl.when(here)
    def _():
        for copy in blocks:
            copy.start()

    for k in far:
        push(share.at[me], share.at[me], s_sh.at[k], r_sh.at[me], flipped(me, k), core)

    for j in range(group):
        for s in range(tp):
            arrive(gotp.at[s * group + j], r_part.at[s * group + j])
        for i in range(3):
            total = gotp[j, i].astype(jnp.float32)
            for s in range(1, tp):
                total = total + gotp[s * group + j, i].astype(jnp.float32)
            total = total.astype(jnp.bfloat16).astype(jnp.float32)
            by_head((query, key, value)[i], total, j * (cols // LANE_WIDTH))

    wide = pack * LANE_WIDTH
    placed = lax.rem(
        lax.broadcasted_iota(jnp.int32, (heads, wide), 0), pack
    ) == lax.broadcasted_iota(jnp.int32, (heads, wide), 1) // LANE_WIDTH
    vlane = lax.broadcasted_iota(jnp.int32, (LANE_WIDTH, 128), 1)
    turn = lax.rem(vlane, heads) // pack

    def spread(channels):
        return jnp.where(placed, jnp.concatenate([channels] * pack, axis=-1), 0.0).astype(
            jnp.bfloat16
        )

    for b in range(own):
        q, k, v, r = query[b], key[b], value[b], rate[b]
        unit = k * lax.rsqrt(jnp.sum(k * k, axis=-1, keepdims=True) + 1.0)
        scaled, pulled, seen = k * r, unit * r, decay[b] * q
        flip[b, 2 * heads : 3 * heads] = v
        probes[b, 0:heads] = spread(unit)
        probes[b, heads : 2 * heads] = spread(seen)
        moves[b, 0:heads] = spread(-pulled)
        moves[b, 2 * heads : 3 * heads] = spread(scaled)
        value_cols = flip[b].T
        sums = across_dot(pk16[b], probes[b])
        found = jnp.zeros((LANE_WIDTH, 128), jnp.float32)
        for p in range(packs):
            at = slice(p * LANE_WIDTH, (p + 1) * LANE_WIDTH)
            both = jnp.where(vlane < 2 * heads, sums[at], value_cols)
            both = jnp.where(turn == p, both, 0.0)
            factors[b, at] = both.astype(jnp.bfloat16)
            found = found + both
        turned = found.T
        seen_rows = (
            turned[heads : 2 * heads]
            - turned[0:heads] * jnp.sum(pulled * q, axis=-1, keepdims=True)
            + v * jnp.sum(scaled * q, axis=-1, keepdims=True)
        )
        centred = seen_rows - jnp.mean(seen_rows, axis=-1, keepdims=True)
        level = lax.rsqrt(jnp.mean(centred * centred, axis=-1, keepdims=True) + GROUP_EPS)
        extra = jnp.sum(q * scaled * reward[...], axis=-1, keepdims=True) * v
        read[b] = centred * level * lane_gain[...] + extra
    for h in range(0, heads, 2):
        joined = jnp.concatenate([read[:, h + i, :] for i in range(2)], axis=-1)
        att[:, h * LANE_WIDTH : (h + 2) * LANE_WIDTH] = joined.astype(jnp.bfloat16)
    for k in far:
        push(att, att_all.at[me], s_att.at[k], r_att.at[me], flipped(me, k), core)
    att_all[me] = att[...]

    def renew(b, _):
        change = jnp.dot(factors[b], moves[b], preferred_element_type=jnp.float32)
        for p in range(packs):
            at = slice(p * LANE_WIDTH, (p + 1) * LANE_WIDTH)
            new = pk[b, at] * dch[pl.ds(b, 1), p * wide : (p + 1) * wide] + change[at]
            for i in range(pack):
                mem[b, p * pack + i] = new[:, i * LANE_WIDTH : (i + 1) * LANE_WIDTH]
        return _

    lax.fori_loop(0, own, renew, 0)

    weights[3].wait()
    for k in far:
        e = flipped(me, k)
        arrive(att_all.at[e], r_att.at[e])
    done = jnp.dot(
        att_all[...].reshape(rows, half), wo[...], preferred_element_type=jnp.float32
    ).astype(jnp.bfloat16)
    pbuf[...] = done.reshape(tp, group * own, cols)
    push(pbuf.at[mate], psib, s_p, r_p, me, mate)
    for j in range(group):
        e = core * group + j

        @pl.when(e != me)
        def _():
            arrive(xcol.at[e], r_x.at[e])

    arrive(psib, r_p)
    mixed = (pbuf[core].astype(jnp.float32) + psib[...].astype(jnp.float32)).astype(jnp.bfloat16)
    held = xcol[pl.ds(core * group, group)].reshape(group * own, cols).astype(jnp.float32)
    res[me, core] = (held + mixed.astype(jnp.float32)).astype(jnp.bfloat16)
    for k in far:
        push(res.at[me, core], res.at[me, core], s_res.at[k], r_res.at[me], flipped(me, k), core)
    push(res.at[me, core], res.at[me, core], f_res.at[me], b_res.at[me], me, mate)
    for k in reversed(far):
        e = flipped(me, k)
        arrive(res.at[e, core], r_res.at[e])
        push(res.at[e, core], res.at[e, core], f_res.at[e], b_res.at[e], me, mate)
    for k in reversed([*far, 0]):
        e = flipped(me, k)
        arrive(res.at[e, mate], b_res.at[e])
    square = jnp.zeros((rows, 1), jnp.float32)
    for s in range(ep):
        block = res[s].reshape(rows, cols).astype(jnp.float32)
        square = square + jnp.sum(block * block, axis=-1, keepdims=True)
    inv = lax.rsqrt(square / width + RMS_EPS)
    switch = cs[...].astype(jnp.float32)
    gate_sum = jnp.zeros((rows, 1), jnp.float32)
    for s in range(ep):
        at = slice(s * cols, (s + 1) * cols)
        block = res[s].reshape(rows, cols).astype(jnp.float32)
        block = (block * inv * gain2[:, at]).astype(jnp.bfloat16)
        ffn[:, at] = block
        block = block.astype(jnp.float32)
        for i in range(cols // 128):
            line = s * (cols // 128) + i
            part_of = block[:, i * 128 : (i + 1) * 128] * switch[line : line + 1]
            gate_sum = gate_sum + jnp.sum(part_of, axis=-1, keepdims=True)
    branch_scale = 1.0 / (1.0 + jnp.exp(-gate_sum))
    for k in far:
        e = flipped(me, k)
        arrive(share.at[e], r_sh.at[e])
    expert = (me * tp + core) * wg.shape[1] // expert_cols
    table = share[...].astype(jnp.float32).reshape(rows, 128)
    picked = lax.broadcasted_iota(jnp.int32, (rows, 128), 1) == expert
    weight = jnp.sum(jnp.where(picked, table, 0.0), axis=-1, keepdims=True)
    for copy in weights[4:6]:
        copy.wait()

    def widen_up(c, _):
        at = pl.ds(pl.multiple_of(c * 256, 256), 256)
        g = jnp.dot(ffn[...], wg[:, at], preferred_element_type=jnp.float32)
        u = jnp.dot(ffn[...], wu[:, at], preferred_element_type=jnp.float32)
        hid[:, at] = (g / (1.0 + jnp.exp(-g)) * u).astype(jnp.bfloat16)
        return _

    lax.fori_loop(0, wg.shape[1] // 256, widen_up, 0)
    for copy in weights[6:8]:
        copy.wait()
    g, u = across_dot(ffn[...], cg[...]), across_dot(ffn[...], cu[...])
    chid[...] = (g / (1.0 + jnp.exp(-g)) * u).astype(jnp.bfloat16)
    for copy in weights[8:]:
        copy.wait()
    pieces = mine.shape[0]
    piece = width // pieces
    last = own // tp
    for n in range(pieces):
        at = slice(n * piece, (n + 1) * piece)
        y = weight * jnp.dot(hid[...], wd[:, at], preferred_element_type=jnp.float32)
        y = y + branch_scale * jnp.dot(chid[...], cd[:, at], preferred_element_type=jnp.float32)
        y = y.reshape(ep, tp, last, piece)
        for i in range(tp):
            sibout[n, i] = y[:, i].astype(jnp.bfloat16)
        push(sibout.at[n, mate], sibin.at[n], s_sib.at[n], r_sib.at[n], me, mate)
    for n in range(pieces):
        arrive(sibin.at[n], r_sib.at[n])
        mine[n] = (
            sibout[n, core].astype(jnp.float32) + sibin[n].astype(jnp.float32)
        ).astype(jnp.bfloat16)
        for k in far:
            e = flipped(me, k)
            push(mine.at[n, e], got.at[n, me], s_out.at[n, k], r_out.at[n, me], e, core)
    start = pl.multiple_of(lax.rem(me, group) * own, own)
    per = piece // cols
    for n in range(pieces):
        total = mine[n, me].astype(jnp.float32)
        for k in reversed(far):
            e = flipped(me, k)
            arrive(got.at[n, e], r_out.at[n, e])
            total = total + got[n, e].astype(jnp.float32)
        for s in range(per):
            base = res[n * per + s, side, pl.ds(start, own)].astype(jnp.float32)
            base = jnp.where(core == 0, base[:last], base[last:])
            a = n * piece + s * cols
            out[:, a : a + cols] = (base + total[:, s * cols : (s + 1) * cols]).astype(jnp.bfloat16)
    for send in sends:
        send.wait_send()

    @pl.when(jnp.logical_not(here))
    def _():
        across.wait_send()

    @pl.when(here)
    def _():
        for copy in blocks:
            copy.wait_send()


def layer(*blocks):
    own = blocks[0].shape[0]
    cols, hidden = blocks[9].shape[1], blocks[18].shape[1]
    heads = blocks[17].shape[0]
    tiles = cols % 128 == 0 and hidden % 256 == 0 and own % 16 == 0
    tiles = tiles and heads % 8 == 0 and 128 % heads == 0 and heads <= 32
    tiles = tiles and blocks[0].shape[1] % 2048 == 0 and cols % 256 == 0
    ep = lax.axis_size("ep")
    heads_match = ep & (ep - 1) == 0 and ep % 2 == 0 and lax.axis_size("tp") == 2
    weights = sum(2 * w.size for w in blocks[18:24])
    rows = own * ep
    held = weights + rows * (12 * blocks[0].shape[1] + 8 * hidden) + 14 * blocks[1].size
    small = held < VMEM_ROOM
    return (kernel_body if tiles and heads_match and small else body)(*blocks)


def kernel_body(
    fresh_inputs,
    memory_arrays,
    chosen_specialist,
    chosen_coefficient,
    first_rescale,
    second_rescale,
    receiver_projector,
    address_projector,
    content_projector,
    final_projector,
    forget_narrowing,
    forget_widening,
    forget_bias,
    learning_narrowing,
    learning_widening,
    learning_bias,
    lane_scaling,
    instant_reward,
    specialist_switch,
    specialist_expand,
    specialist_contract,
    common_activator,
    common_expand,
    common_contract,
    common_switch,
):
    ep, tp = lax.axis_size("ep"), lax.axis_size("tp")
    own, width = fresh_inputs.shape
    half, cols = width // tp, final_projector.shape[1]
    heads = half // LANE_WIDTH
    group = ep // tp
    vmem = pl.BlockSpec(memory_space=pltpu.VMEM)
    hbm = pl.BlockSpec(memory_space=pl.ANY)
    bf16, f32 = jnp.bfloat16, jnp.float32
    dma = pltpu.SemaphoreType.DMA

    def row(vector):
        return vector.reshape(1, -1)

    rows, hidden, dense = ep * own, specialist_switch.shape[1], common_activator.shape[1]
    low, top = forget_narrowing.shape[1], chosen_specialist.shape[1]
    pack = 4
    wide, block_rows = pack * LANE_WIDTH, heads // pack * LANE_WIDTH
    pieces, batches = 4, 4
    piece, last = width // pieces, own // tp
    per_head = pltpu.VMEM((own, heads, LANE_WIDTH), f32)
    new_tokens, memory_after = pl.pallas_call(
        functools.partial(layer_kernel, ep, tp, FF_E),
        out_shape=(
            pltpu.VMEM((last, width), bf16),
            pltpu.VMEM(memory_arrays.shape, f32),
        ),
        in_specs=[hbm] * 25,
        out_specs=(vmem, vmem),
        scratch_shapes=[
            pltpu.VMEM((own, width), bf16),
            pltpu.VMEM((top, own), jnp.int32),
            pltpu.VMEM((top, own), bf16),
            pltpu.VMEM((1, width), f32),
            pltpu.VMEM((1, width), f32),
            pltpu.VMEM((width // 128, 128), bf16),
            pltpu.VMEM((heads, LANE_WIDTH), f32),
            pltpu.VMEM((1, half), f32),
            pltpu.VMEM((low, width), bf16),
            pltpu.VMEM((low, half), bf16),
            pltpu.VMEM((1, half), f32),
            pltpu.VMEM((low, width), bf16),
            pltpu.VMEM((low, half), bf16),
            pltpu.VMEM((1, half), f32),
            pltpu.VMEM((3, half, cols), bf16),
            pltpu.VMEM((half, cols), bf16),
            pltpu.VMEM((width, hidden), bf16),
            pltpu.VMEM((width, hidden), bf16),
            pltpu.VMEM((hidden, width), bf16),
            pltpu.VMEM((dense, width), bf16),
            pltpu.VMEM((dense, width), bf16),
            pltpu.VMEM((dense, width), bf16),
            pltpu.VMEM((own, block_rows, wide), f32),
            pltpu.VMEM((own, block_rows, wide), bf16),
            pltpu.VMEM((tp, own, half), bf16),
            pltpu.VMEM((ep, own, half), bf16),
            pltpu.VMEM((ep, 3, own, cols), bf16),
            pltpu.VMEM((ep, 3, own, cols), bf16),
            per_head,
            per_head,
            per_head,
            per_head,
            per_head,
            pltpu.VMEM((own, half), f32),
            pltpu.VMEM((heads, LANE_WIDTH), f32),
            pltpu.VMEM((own, 128, LANE_WIDTH), f32),
            pltpu.VMEM((own, 128, wide), bf16),
            pltpu.VMEM((own, 128, wide), bf16),
            pltpu.VMEM((own, block_rows, 128), bf16),
            per_head,
            pltpu.VMEM((own, half), bf16),
            pltpu.VMEM((ep, own, half), bf16),
            pltpu.VMEM((ep, own, cols), bf16),
            pltpu.VMEM((ep, own, 128), bf16),
            pltpu.VMEM((tp, group * own, cols), bf16),
            pltpu.VMEM((group * own, cols), bf16),
            pltpu.VMEM((ep, tp, group * own, cols), bf16),
            pltpu.VMEM((rows, width), bf16),
            pltpu.VMEM((rows, hidden), bf16),
            pltpu.VMEM((rows, dense), bf16),
            pltpu.VMEM((pieces, tp, ep, last, piece), bf16),
            pltpu.VMEM((pieces, ep, last, piece), bf16),
            pltpu.VMEM((pieces, ep, last, piece), bf16),
            pltpu.VMEM((pieces, ep, last, piece), bf16),
            dma((14,)),
            dma((batches,)),
            dma((10,)),
            *[dma((ep,))] * 10,
            dma,
            dma,
            *[dma((ep,))] * 4,
            dma((pieces,)),
            dma((pieces,)),
            dma((pieces, ep)),
            dma((pieces, ep)),
        ],
        compiler_params=pltpu.CompilerParams(
            collective_id=0, has_side_effects=True, vmem_limit_bytes=54 * 2**20
        ),
        name="layer",
    )(
        fresh_inputs,
        memory_arrays,
        chosen_specialist.T,
        chosen_coefficient.T,
        row(first_rescale),
        row(second_rescale),
        common_switch.reshape(-1, 128),
        instant_reward,
        row(lane_scaling),
        receiver_projector,
        address_projector,
        content_projector,
        final_projector,
        forget_narrowing.T,
        forget_widening,
        row(forget_bias),
        learning_narrowing.T,
        learning_widening,
        row(learning_bias),
        specialist_switch,
        specialist_expand,
        specialist_contract,
        common_activator.T,
        common_expand.T,
        common_contract,
    )
    return (new_tokens, memory_after)


def solution(mesh):
    placed = (
        P(("grp", "ep"), None),
        P(("grp", "ep"), "tp", None, None),
        P(("grp", "ep"), None),
        P(("grp", "ep"), None),
        P(),
        P(),
        P("tp", "ep"),
        P("tp", "ep"),
        P("tp", "ep"),
        P("tp", "ep"),
        P(),
        P(None, "tp"),
        P("tp"),
        P(),
        P(None, "tp"),
        P("tp"),
        P("tp"),
        P("tp", None),
        P(None, ("ep", "tp")),
        P(None, ("ep", "tp")),
        P(("ep", "tp"), None),
        P(None, ("ep", "tp")),
        P(None, ("ep", "tp")),
        P(("ep", "tp"), None),
        P(),
    )
    return jax.shard_map(
        layer,
        mesh=mesh,
        in_specs=placed,
        out_specs=(P(("grp", "ep", "tp"), None), P(("grp", "ep"), "tp", None, None)),
        check_vma=False,
    )
```

```python
import functools
import math

import jax
import jax.numpy as jnp
from jax import lax
from jax.experimental import pallas as pl
from jax.experimental.pallas import tpu as pltpu
from jax.sharding import PartitionSpec as P

LANE_WIDTH = 64
FF_E = 7168


RMS_EPS = 1e-06
GROUP_EPS = 0.00064
HIGHEST = lax.Precision.HIGHEST
MESH = pl.DeviceIdType.MESH
VMEM_ROOM = 52 * 2**20


def rms_norm(values, norm_gain):
    mean_sq = jnp.mean(values * values, axis=-1, keepdims=True)
    return values * lax.rsqrt(mean_sq + RMS_EPS) * norm_gain


def widen(rounded):
    return lax.optimization_barrier(rounded).astype(jnp.float32)


def evolve_memory(
    memory_arrays,
    receiver_lanes,
    address_lanes,
    content_lanes,
    forget_lanes,
    learning_lanes,
    lane_rescale,
    instant_reward,
):
    unit_key = address_lanes * lax.rsqrt(
        jnp.sum(address_lanes * address_lanes, axis=-1, keepdims=True) + 1.0
    )
    stepped_address = address_lanes * learning_lanes
    removal = jnp.einsum("bhvk,bhk->bhv", memory_arrays, unit_key, precision=HIGHEST)
    memory_after = (
        memory_arrays * forget_lanes[:, :, None, :]
        - removal[..., None] * (unit_key * learning_lanes)[:, :, None, :]
        + content_lanes[..., None] * stepped_address[:, :, None, :]
    )
    memory_retrieval = jnp.einsum("bhvk,bhk->bhv", memory_after, receiver_lanes, precision=HIGHEST)
    centred = memory_retrieval - jnp.mean(memory_retrieval, axis=-1, keepdims=True)
    unit_address = centred * lax.rsqrt(
        jnp.mean(centred * centred, axis=-1, keepdims=True) + GROUP_EPS
    )
    instant_extra = (
        jnp.sum(receiver_lanes * stepped_address * instant_reward, axis=-1, keepdims=True)
        * content_lanes
    )
    return (memory_after, unit_address * lane_rescale + instant_extra)


def swiglu(rows_in, gate_w, up_w):
    gate_val = jnp.dot(rows_in, gate_w, preferred_element_type=jnp.float32)
    up_val = jnp.dot(rows_in, up_w, preferred_element_type=jnp.float32)
    return (jax.nn.silu(gate_val) * up_val).astype(jnp.bfloat16)


def body(
    fresh_inputs,
    memory_arrays,
    chosen_specialist,
    chosen_coefficient,
    first_rescale,
    second_rescale,
    receiver_projector,
    address_projector,
    content_projector,
    final_projector,
    forget_narrowing,
    forget_widening,
    forget_bias,
    learning_narrowing,
    learning_widening,
    learning_bias,
    lane_scaling,
    instant_reward,
    specialist_switch,
    specialist_expand,
    specialist_contract,
    common_activator,
    common_expand,
    common_contract,
    common_switch,
):
    own_rows = fresh_inputs.shape[0]
    model_width = fresh_inputs.shape[1]
    tp_count = lax.axis_size("tp")
    tp_rank = lax.axis_index("tp")
    half_width = model_width // tp_count
    head_count = half_width // LANE_WIDTH
    residual = fresh_inputs.astype(jnp.float32)
    normed = rms_norm(residual, first_rescale).astype(jnp.bfloat16)
    normed_half = lax.dynamic_slice_in_dim(normed, tp_rank * half_width, half_width, 1)
    local_weights = jnp.stack((receiver_projector, address_projector, content_projector), axis=1)
    projected_rows = jnp.einsum(
        "rd,dkc->rkc",
        lax.all_gather(normed_half, "ep", axis=0, tiled=True),
        local_weights,
        preferred_element_type=jnp.float32,
    ).astype(jnp.bfloat16)
    partial_value = lax.all_to_all(projected_rows, "ep", split_axis=0, concat_axis=2, tiled=True)
    projected = lax.psum(widen(partial_value).astype(jnp.bfloat16), "tp")
    mine = lax.dynamic_slice_in_dim(projected, tp_rank * half_width, half_width, 2)

    def divide_lanes(channels):
        return channels.astype(jnp.float32).reshape(own_rows, head_count, LANE_WIDTH)

    decay_mid = jnp.tanh(
        jnp.dot(normed, forget_narrowing, preferred_element_type=jnp.float32)
    ).astype(jnp.bfloat16)
    decay_pre = forget_bias + jnp.dot(
        decay_mid, forget_widening, preferred_element_type=jnp.float32
    )
    decay_vals = jnp.exp(-jnp.exp(-jax.nn.softplus(-decay_pre) - 0.5))
    rate_mid = jnp.dot(normed, learning_narrowing, preferred_element_type=jnp.float32).astype(
        jnp.bfloat16
    )
    rate_vals = jax.nn.sigmoid(
        learning_bias + jnp.dot(rate_mid, learning_widening, preferred_element_type=jnp.float32)
    )
    memory_after, memory_retrieval = evolve_memory(
        memory_arrays,
        divide_lanes(mine[:, 0]),
        divide_lanes(mine[:, 1]),
        divide_lanes(mine[:, 2]),
        divide_lanes(decay_vals),
        divide_lanes(rate_vals),
        lane_scaling.reshape(head_count, LANE_WIDTH),
        instant_reward,
    )
    attended = memory_retrieval.reshape(own_rows, half_width).astype(jnp.bfloat16)
    done_rows = jnp.dot(
        lax.all_gather(attended, "ep", axis=0, tiled=True),
        final_projector,
        preferred_element_type=jnp.float32,
    ).astype(jnp.bfloat16)
    out_part = lax.all_to_all(done_rows, "ep", split_axis=0, concat_axis=1, tiled=True)
    mixed_out = lax.psum(widen(out_part).astype(jnp.bfloat16), "tp")
    residual = residual + mixed_out.astype(jnp.float32)
    ffn_in = rms_norm(residual, second_rescale).astype(jnp.bfloat16)
    all_in, all_weight, all_ids = (
        lax.all_gather(ffn_in, "ep", axis=0, tiled=True),
        lax.all_gather(chosen_coefficient, "ep", axis=0, tiled=True),
        lax.all_gather(chosen_specialist, "ep", axis=0, tiled=True),
    )
    column_count = specialist_switch.shape[1]
    flat_rank = lax.axis_index("ep") * tp_count + tp_rank
    expert = flat_rank * column_count // FF_E
    expert_share = jnp.sum(
        jnp.where(all_ids == expert, all_weight.astype(jnp.float32), 0.0), axis=1
    )
    hidden = swiglu(all_in, specialist_switch, specialist_expand)
    shared_hidden = swiglu(all_in, common_activator, common_expand)
    branch_scale = jax.nn.sigmoid(
        jnp.dot(all_in, common_switch, preferred_element_type=jnp.float32)
    )
    rows_mine = own_rows // tp_count
    expert_term = expert_share[:, None] * jnp.dot(
        hidden, specialist_contract, preferred_element_type=jnp.float32
    )
    routed = lax.psum_scatter(
        expert_term
        + branch_scale[:, None]
        * jnp.dot(shared_hidden, common_contract, preferred_element_type=jnp.float32),
        ("ep", "tp"),
        scatter_dimension=0,
        tiled=True,
    )
    own_residual = lax.dynamic_slice_in_dim(residual, tp_rank * rows_mine, rows_mine, 0)
    return ((own_residual + routed).astype(jnp.bfloat16), memory_after)


def flipped(index, mask, count):
    total, step = 0, 1
    while step < count:
        total = total + step * lax.rem(index // step + mask // step, 2)
        step = 2 * step
    return total


def _greet(ep, tp):
    me, core = lax.axis_index("ep"), lax.axis_index("tp")
    barrier = pltpu.get_barrier_semaphore()
    for mask in range(ep - 1, -1, -1):
        for side in range(tp):
            if mask or side:
                pl.semaphore_signal(
                    barrier,
                    inc=1,
                    device_id={"ep": flipped(me, mask, ep), "tp": lax.rem(core + side, tp)},
                    device_id_type=MESH,
                )


def _met(ep, tp):
    pl.semaphore_wait(pltpu.get_barrier_semaphore(), ep * tp - 1)


def _remote(src, dst, send, recv, e, t):
    return pltpu.make_async_remote_copy(
        src_ref=src,
        dst_ref=dst,
        send_sem=send,
        recv_sem=recv,
        device_id={"ep": e, "tp": t},
        device_id_type=MESH,
    )


def across_dot(left, right):
    return lax.dot_general(
        left, right, (((1,), (1,)), ((), ())), preferred_element_type=jnp.float32
    )


def by_head(ref, channels, first):
    for h in range(channels.shape[1] // LANE_WIDTH):
        ref[:, first + h, :] = channels[:, h * LANE_WIDTH : (h + 1) * LANE_WIDTH]


def arrive(ref, sem):
    pltpu.make_async_copy(ref, ref, sem).wait()


def layer_kernel(
    ep, tp, expert_cols,
    x_h, memory, ids_h, coef_h, gain_h, gain2_h, cs_h, reward_h, scaling_h,
    wq_h, wk_h, wv_h, wo_h, fnar_h, fwid_h, fbias_h, lnar_h, lwid_h, lbias_h,
    wg_h, wu_h, wd_h, cg_h, cu_h, cd_h,
    out, mem,
    x, ids, coef, gain, gain2, cs16, cs, reward, scaling, fnar, fwid, fbias, lnar, lwid, lbias,
    w, wo, wg, wu, wd, cg, cu, cd, pk, pk16,
    halves, rows_all, part, gotp, query, key, value, decay, rate, dch, lane_gain,
    flip, probes, moves, factors, read,
    att, att_all, xcol, share, pbuf, psib, res, gacc, uacc, cgacc, cuacc, sq, gs, hid, chid, sibout, sibin, mine, got,
    lsem, msem, wsem,
    s_row, r_row, s_part, r_part, s_att, r_att, s_x, r_x, s_sh, r_sh, s_p, r_p,
    s_res, r_res, f_res, b_res, s_sib, r_sib, s_out, r_out,
):
    me, core = lax.axis_index("ep"), lax.axis_index("tp")
    mate = lax.rem(core + 1, tp)
    group = ep // tp
    side = me // group
    own, width = x.shape
    half = width // tp
    cols = wo.shape[1]
    rows = ep * own
    heads = lane_gain.shape[0]
    pack = pk.shape[2] // LANE_WIDTH
    packs = heads // pack
    block_rows = packs * LANE_WIDTH
    far = list(range(1, ep))
    turn_at, turned_by = ep // 2, ep // 2 + 1
    direct = [turn_at] + [k for k in far if k not in (turn_at, turned_by)]
    _greet(ep, tp)

    smalls = [
        pltpu.make_async_copy(a, b, lsem.at[i])
        for i, (a, b) in enumerate(
            (
                (x_h, x), (gain_h, gain), (fnar_h, fnar), (fwid_h, fwid), (fbias_h, fbias),
                (lnar_h, lnar), (lwid_h, lwid), (lbias_h, lbias), (scaling_h, scaling),
                (reward_h, reward), (ids_h, ids), (coef_h, coef), (gain2_h, gain2), (cs_h, cs16),
            )
        )
    ]
    weights = [
        pltpu.make_async_copy(a, b, wsem.at[i])
        for i, (a, b) in enumerate(
            (
                (wq_h, w.at[0]), (wk_h, w.at[1]), (wv_h, w.at[2]), (wo_h, wo), (wg_h, wg),
                (wu_h, wu), (cg_h, cg), (cu_h, cu), (wd_h, wd), (cd_h, cd),
            )
        )
    ]
    batches = msem.shape[0]
    batch = own // batches
    states = [
        pltpu.make_async_copy(
            memory.at[pl.ds(i * batch, batch)], mem.at[pl.ds(i * batch, batch)], msem.at[i]
        )
        for i in range(batches)
    ]
    for copy in smalls + weights[:3] + states:
        copy.start()
    sends = []

    def push(*args):
        sends.append(_remote(*args))
        sends[-1].start()

    def spread_out(block, every, send, recv):
        for k in direct:
            push(block, every.at[me], send.at[k], recv.at[me], flipped(me, k, ep), core)

    def hand_on(every, send, recv):
        e = flipped(me, turn_at, ep)
        arrive(every.at[e], recv.at[e])
        push(every.at[e], every.at[e], send.at[turned_by], recv.at[e], flipped(me, 1, ep), core)

    def gathered(every, recv):
        for k in far:
            if k != turn_at:
                e = flipped(me, k, ep)
                arrive(every.at[e], recv.at[e])

    for copy in smalls[:2]:
        copy.wait()
    normed = rms_norm(x[...].astype(jnp.float32), gain[...]).astype(jnp.bfloat16)
    for i in range(tp):
        halves[i] = normed[:, i * half : (i + 1) * half]
    _met(ep, tp)
    spread_out(halves.at[core], rows_all, s_row, r_row)
    rows_all[me] = halves[core]

    for copy in smalls[2:]:
        copy.wait()
    cs[...] = cs16[...].astype(jnp.float32)
    decay_mid = jnp.tanh(across_dot(normed, fnar[...])).astype(jnp.bfloat16)
    decay_pre = fbias[...] + jnp.dot(decay_mid, fwid[...], preferred_element_type=jnp.float32)
    kept = jnp.exp(-(math.exp(-0.5) / (1.0 + jnp.exp(-decay_pre))))
    dch[...] = kept
    by_head(decay, kept, 0)
    rate_mid = across_dot(normed, lnar[...]).astype(jnp.bfloat16)
    rate_pre = lbias[...] + jnp.dot(rate_mid, lwid[...], preferred_element_type=jnp.float32)
    by_head(rate, 1.0 / (1.0 + jnp.exp(-rate_pre)), 0)
    for h in range(heads):
        lane_gain[h : h + 1] = scaling[:, h * LANE_WIDTH : (h + 1) * LANE_WIDTH]
    for ref in (flip, probes, moves):
        ref[...] = jnp.zeros_like(ref)
    lane = lax.broadcasted_iota(jnp.int32, (own, 128), 1)
    routes = jnp.zeros((own, 128), jnp.float32)
    ids_cols, coef_cols = ids[...].T, coef[...].astype(jnp.float32).T
    for i in range(ids.shape[0]):
        routes = routes + jnp.where(
            ids_cols[:, i : i + 1] == lane, coef_cols[:, i : i + 1], 0.0
        )
    share[me] = routes.astype(jnp.bfloat16)
    xcol[me] = x[:, pl.ds(pl.multiple_of(me * cols, cols), cols)]
    hand_on(rows_all, s_row, r_row)
    for copy in states:
        copy.wait()
    for copy in weights[3:]:
        copy.start()

    def join(b, _):
        for p in range(packs):
            joined = jnp.concatenate([mem[b, p * pack + i] for i in range(pack)], axis=-1)
            at = slice(p * LANE_WIDTH, (p + 1) * LANE_WIDTH)
            pk[b, at] = joined
            pk16[b, at] = joined.astype(jnp.bfloat16)
        return _

    lax.fori_loop(0, own, join, 0)

    for copy in weights[:3]:
        copy.wait()
    gathered(rows_all, r_row)
    every = rows_all[...].reshape(rows, half)
    for i in range(3):
        done = jnp.dot(every, w[i], preferred_element_type=jnp.float32)
        part[:, i] = done.astype(jnp.bfloat16).reshape(ep, own, cols)
    slot = core * group + lax.rem(me, group)
    for k in far:
        e = flipped(me, k, ep)
        push(part.at[e], gotp.at[slot], s_part.at[k], r_part.at[slot], e, side)
    here = side == core
    local = pltpu.make_async_copy(part.at[me], gotp.at[slot], r_part.at[slot])
    across = _remote(part.at[me], gotp.at[slot], s_part.at[0], r_part.at[slot], me, side)

    @pl.when(here)
    def _():
        local.start()

    @pl.when(jnp.logical_not(here))
    def _():
        across.start()

    blocks = []
    for k in far:
        e = flipped(me, k, ep)
        block = x.at[:, pl.ds(pl.multiple_of(e * cols, cols), cols)]
        blocks.append(_remote(block, xcol.at[me], s_x.at[k], r_x.at[me], e, core))

    @pl.when(here)
    def _():
        for copy in blocks:
            copy.start()

    for k in far:
        push(share.at[me], share.at[me], s_sh.at[k], r_sh.at[me], flipped(me, k, ep), core)

    for j in range(group):
        for s in range(tp):
            arrive(gotp.at[s * group + j], r_part.at[s * group + j])
        for i in range(3):
            total = gotp[j, i].astype(jnp.float32)
            for s in range(1, tp):
                total = total + gotp[s * group + j, i].astype(jnp.float32)
            total = total.astype(jnp.bfloat16).astype(jnp.float32)
            by_head((query, key, value)[i], total, j * (cols // LANE_WIDTH))

    wide = pack * LANE_WIDTH
    placed = lax.rem(
        lax.broadcasted_iota(jnp.int32, (heads, wide), 0), pack
    ) == lax.broadcasted_iota(jnp.int32, (heads, wide), 1) // LANE_WIDTH
    vlane = lax.broadcasted_iota(jnp.int32, (LANE_WIDTH, 128), 1)
    turn = lax.rem(vlane, heads) // pack

    def spread(channels):
        return jnp.where(placed, jnp.concatenate([channels] * pack, axis=-1), 0.0).astype(
            jnp.bfloat16
        )

    for b in range(own):
        q, k, v, r = query[b], key[b], value[b], rate[b]
        unit = k * lax.rsqrt(jnp.sum(k * k, axis=-1, keepdims=True) + 1.0)
        scaled, pulled, seen = k * r, unit * r, decay[b] * q
        flip[b, 2 * heads : 3 * heads] = v
        probes[b, 0:heads] = spread(unit)
        probes[b, heads : 2 * heads] = spread(seen)
        moves[b, 0:heads] = spread(-pulled)
        moves[b, 2 * heads : 3 * heads] = spread(scaled)
        value_cols = flip[b].T
        sums = across_dot(pk16[b], probes[b])
        found = jnp.zeros((LANE_WIDTH, 128), jnp.float32)
        for p in range(packs):
            at = slice(p * LANE_WIDTH, (p + 1) * LANE_WIDTH)
            both = jnp.where(vlane < 2 * heads, sums[at], value_cols)
            both = jnp.where(turn == p, both, 0.0)
            factors[b, at] = both.astype(jnp.bfloat16)
            found = found + both
        turned = found.T
        seen_rows = (
            turned[heads : 2 * heads]
            - turned[0:heads] * jnp.sum(pulled * q, axis=-1, keepdims=True)
            + v * jnp.sum(scaled * q, axis=-1, keepdims=True)
        )
        centred = seen_rows - jnp.mean(seen_rows, axis=-1, keepdims=True)
        level = lax.rsqrt(jnp.mean(centred * centred, axis=-1, keepdims=True) + GROUP_EPS)
        extra = jnp.sum(q * scaled * reward[...], axis=-1, keepdims=True) * v
        read[b] = centred * level * lane_gain[...] + extra
    for h in range(0, heads, 2):
        joined = jnp.concatenate([read[:, h + i, :] for i in range(2)], axis=-1)
        att[:, h * LANE_WIDTH : (h + 2) * LANE_WIDTH] = joined.astype(jnp.bfloat16)
    spread_out(att, att_all, s_att, r_att)
    att_all[me] = att[...]

    def renew(b, _):
        change = jnp.dot(factors[b], moves[b], preferred_element_type=jnp.float32)
        for p in range(packs):
            at = slice(p * LANE_WIDTH, (p + 1) * LANE_WIDTH)
            new = pk[b, at] * dch[pl.ds(b, 1), p * wide : (p + 1) * wide] + change[at]
            for i in range(pack):
                mem[b, p * pack + i] = new[:, i * LANE_WIDTH : (i + 1) * LANE_WIDTH]
        return _

    lax.fori_loop(0, own // 2, renew, 0)
    hand_on(att_all, s_att, r_att)
    lax.fori_loop(own // 2, own, renew, 0)

    weights[3].wait()
    for k in far:
        e = flipped(me, k, ep)
        arrive(share.at[e], r_sh.at[e])
    gathered(att_all, r_att)
    done = jnp.dot(
        att_all[...].reshape(rows, half), wo[...], preferred_element_type=jnp.float32
    ).astype(jnp.bfloat16)
    pbuf[...] = done.reshape(tp, group * own, cols)
    push(pbuf.at[mate], psib, s_p, r_p, me, mate)
    for j in range(group):
        e = core * group + j

        @pl.when(e != me)
        def _():
            arrive(xcol.at[e], r_x.at[e])

    arrive(psib, r_p)
    mixed = (pbuf[core].astype(jnp.float32) + psib[...].astype(jnp.float32)).astype(jnp.bfloat16)
    held = xcol[pl.ds(core * group, group)].reshape(group * own, cols).astype(jnp.float32)
    res[me, core] = (held + mixed.astype(jnp.float32)).astype(jnp.bfloat16)
    for k in direct:
        push(res.at[me, core], res.at[me, core], s_res.at[k], r_res.at[me], flipped(me, k, ep), core)
    _remote(res.at[me, core], res.at[me, core], f_res.at[me], b_res.at[me], me, mate).start()
    for ref in (gacc, uacc, cgacc, cuacc, sq, gs):
        ref[...] = jnp.zeros_like(ref)
    for copy in weights[4:8]:
        copy.wait()

    def forward(e):
        return _remote(res.at[e, core], res.at[e, core], f_res.at[e], b_res.at[e], me, mate)

    def absorb(e):
        arrive(res.at[e, mate], b_res.at[e])
        at = pl.ds(pl.multiple_of(e * cols, cols), cols)
        block = res[e].reshape(rows, cols).astype(jnp.float32)
        scaled = (block * gain2[:, at]).astype(jnp.bfloat16)
        gacc[...] += jnp.dot(scaled, wg[at, :], preferred_element_type=jnp.float32)
        uacc[...] += jnp.dot(scaled, wu[at, :], preferred_element_type=jnp.float32)
        cgacc[...] += across_dot(scaled, cg[:, at])
        cuacc[...] += across_dot(scaled, cu[:, at])
        wide_rows = scaled.astype(jnp.float32)
        for i in range(cols // 128):
            part_of = block[:, i * 128 : (i + 1) * 128]
            sq[...] += part_of * part_of
            line = cs[pl.ds(e * (cols // 128) + i, 1), :]
            gs[...] += wide_rows[:, i * 128 : (i + 1) * 128] * line

    ready = me
    for k in (1, turn_at, *[k for k in range(2, ep) if k not in (turn_at, turned_by)], turned_by):
        e = flipped(me, k, ep)
        arrive(res.at[e, core], r_res.at[e])
        if k == turn_at:
            push(
                res.at[e, core], res.at[e, core], s_res.at[turned_by], r_res.at[e],
                flipped(me, 1, ep), core,
            )
        forward(e).start()
        absorb(ready)
        ready = e
    absorb(ready)
    inv = lax.rsqrt(jnp.sum(sq[...], axis=-1, keepdims=True) / width + RMS_EPS)
    branch_scale = 1.0 / (1.0 + jnp.exp(-inv * jnp.sum(gs[...], axis=-1, keepdims=True)))
    expert = (me * tp + core) * wg.shape[1] // expert_cols
    table = share[...].astype(jnp.float32).reshape(rows, 128)
    picked = lax.broadcasted_iota(jnp.int32, (rows, 128), 1) == expert
    weight = jnp.sum(jnp.where(picked, table, 0.0), axis=-1, keepdims=True)

    def gated(target, gates, ups):
        g, u = gates[...] * inv, ups[...] * inv
        target[...] = (g / (1.0 + jnp.exp(-g)) * u).astype(jnp.bfloat16)

    gated(hid, gacc, uacc)
    gated(chid, cgacc, cuacc)
    for copy in weights[8:]:
        copy.wait()
    pieces = mine.shape[0]
    piece = width // pieces
    last = own // tp

    def finish(n):
        arrive(sibin.at[n], r_sib.at[n])
        mine[n] = (
            sibout[n, core].astype(jnp.float32) + sibin[n].astype(jnp.float32)
        ).astype(jnp.bfloat16)
        for k in far:
            e = flipped(me, k, ep)
            push(mine.at[n, e], got.at[n, me], s_out.at[n, k], r_out.at[n, me], e, core)

    for n in range(pieces):
        at = slice(n * piece, (n + 1) * piece)
        y = weight * jnp.dot(hid[...], wd[:, at], preferred_element_type=jnp.float32)
        y = y + branch_scale * jnp.dot(chid[...], cd[:, at], preferred_element_type=jnp.float32)
        y = y.reshape(ep, tp, last, piece)
        for i in range(tp):
            sibout[n, i] = y[:, i].astype(jnp.bfloat16)
        push(sibout.at[n, mate], sibin.at[n], s_sib.at[n], r_sib.at[n], me, mate)
        if n:
            finish(n - 1)
    finish(pieces - 1)
    start = pl.multiple_of(lax.rem(me, group) * own, own)
    per = piece // cols
    for n in range(pieces):
        total = mine[n, me].astype(jnp.float32)
        for k in reversed(far):
            e = flipped(me, k, ep)
            arrive(got.at[n, e], r_out.at[n, e])
            total = total + got[n, e].astype(jnp.float32)
        for s in range(per):
            base = res[n * per + s, side, pl.ds(start, own)].astype(jnp.float32)
            base = jnp.where(core == 0, base[:last], base[last:])
            a = n * piece + s * cols
            out[:, a : a + cols] = (base + total[:, s * cols : (s + 1) * cols]).astype(jnp.bfloat16)
    for send in sends:
        send.wait_send()
    for e in range(ep):
        forward(e).wait_send()

    @pl.when(jnp.logical_not(here))
    def _():
        across.wait_send()

    @pl.when(here)
    def _():
        for copy in blocks:
            copy.wait_send()


def settle_kernel(tokens, state, out, after, sems):
    step = state.shape[0] // (sems.shape[0] - 1)
    copies = [pltpu.make_async_copy(tokens, out, sems.at[0])]
    for i in range(sems.shape[0] - 1):
        at = pl.ds(i * step, step)
        copies.append(pltpu.make_async_copy(state.at[at], after.at[at], sems.at[i + 1]))
    for copy in copies:
        copy.start()
    for copy in copies:
        copy.wait()


def layer(*blocks):
    own = blocks[0].shape[0]
    cols, hidden = blocks[9].shape[1], blocks[18].shape[1]
    heads = blocks[17].shape[0]
    tiles = cols % 128 == 0 and hidden % 256 == 0 and own % 16 == 0
    tiles = tiles and heads % 8 == 0 and 128 % heads == 0 and heads <= 32
    tiles = tiles and blocks[0].shape[1] % 2048 == 0 and cols % 256 == 0
    ep = lax.axis_size("ep")
    heads_match = ep & (ep - 1) == 0 and ep > 2 and lax.axis_size("tp") == 2
    weights = sum(2 * w.size for w in blocks[18:24])
    rows = own * ep
    held = weights + rows * (12 * blocks[0].shape[1] + 8 * hidden) + 14 * blocks[1].size
    small = held < VMEM_ROOM
    return (kernel_body if tiles and heads_match and small else body)(*blocks)


def kernel_body(
    fresh_inputs,
    memory_arrays,
    chosen_specialist,
    chosen_coefficient,
    first_rescale,
    second_rescale,
    receiver_projector,
    address_projector,
    content_projector,
    final_projector,
    forget_narrowing,
    forget_widening,
    forget_bias,
    learning_narrowing,
    learning_widening,
    learning_bias,
    lane_scaling,
    instant_reward,
    specialist_switch,
    specialist_expand,
    specialist_contract,
    common_activator,
    common_expand,
    common_contract,
    common_switch,
):
    ep, tp = lax.axis_size("ep"), lax.axis_size("tp")
    own, width = fresh_inputs.shape
    half, cols = width // tp, final_projector.shape[1]
    heads = half // LANE_WIDTH
    group = ep // tp
    vmem = pl.BlockSpec(memory_space=pltpu.VMEM)
    hbm = pl.BlockSpec(memory_space=pl.ANY)
    bf16, f32 = jnp.bfloat16, jnp.float32
    dma = pltpu.SemaphoreType.DMA

    def row(vector):
        return vector.reshape(1, -1)

    rows, hidden, dense = ep * own, specialist_switch.shape[1], common_activator.shape[1]
    low, top = forget_narrowing.shape[1], chosen_specialist.shape[1]
    pack = 4
    wide, block_rows = pack * LANE_WIDTH, heads // pack * LANE_WIDTH
    pieces, batches = 4, 4
    piece, last = width // pieces, own // tp
    per_head = pltpu.VMEM((own, heads, LANE_WIDTH), f32)
    new_tokens, memory_after = pl.pallas_call(
        functools.partial(layer_kernel, ep, tp, FF_E),
        out_shape=(
            pltpu.VMEM((last, width), bf16),
            pltpu.VMEM(memory_arrays.shape, f32),
        ),
        in_specs=[hbm] * 25,
        out_specs=(vmem, vmem),
        scratch_shapes=[
            pltpu.VMEM((own, width), bf16),
            pltpu.VMEM((top, own), jnp.int32),
            pltpu.VMEM((top, own), bf16),
            pltpu.VMEM((1, width), f32),
            pltpu.VMEM((1, width), f32),
            pltpu.VMEM((width // 128, 128), bf16),
            pltpu.VMEM((width // 128, 128), f32),
            pltpu.VMEM((heads, LANE_WIDTH), f32),
            pltpu.VMEM((1, half), f32),
            pltpu.VMEM((low, width), bf16),
            pltpu.VMEM((low, half), bf16),
            pltpu.VMEM((1, half), f32),
            pltpu.VMEM((low, width), bf16),
            pltpu.VMEM((low, half), bf16),
            pltpu.VMEM((1, half), f32),
            pltpu.VMEM((3, half, cols), bf16),
            pltpu.VMEM((half, cols), bf16),
            pltpu.VMEM((width, hidden), bf16),
            pltpu.VMEM((width, hidden), bf16),
            pltpu.VMEM((hidden, width), bf16),
            pltpu.VMEM((dense, width), bf16),
            pltpu.VMEM((dense, width), bf16),
            pltpu.VMEM((dense, width), bf16),
            pltpu.VMEM((own, block_rows, wide), f32),
            pltpu.VMEM((own, block_rows, wide), bf16),
            pltpu.VMEM((tp, own, half), bf16),
            pltpu.VMEM((ep, own, half), bf16),
            pltpu.VMEM((ep, 3, own, cols), bf16),
            pltpu.VMEM((ep, 3, own, cols), bf16),
            per_head,
            per_head,
            per_head,
            per_head,
            per_head,
            pltpu.VMEM((own, half), f32),
            pltpu.VMEM((heads, LANE_WIDTH), f32),
            pltpu.VMEM((own, 128, LANE_WIDTH), f32),
            pltpu.VMEM((own, 128, wide), bf16),
            pltpu.VMEM((own, 128, wide), bf16),
            pltpu.VMEM((own, block_rows, 128), bf16),
            per_head,
            pltpu.VMEM((own, half), bf16),
            pltpu.VMEM((ep, own, half), bf16),
            pltpu.VMEM((ep, own, cols), bf16),
            pltpu.VMEM((ep, own, 128), bf16),
            pltpu.VMEM((tp, group * own, cols), bf16),
            pltpu.VMEM((group * own, cols), bf16),
            pltpu.VMEM((ep, tp, group * own, cols), bf16),
            pltpu.VMEM((rows, hidden), f32),
            pltpu.VMEM((rows, hidden), f32),
            pltpu.VMEM((rows, dense), f32),
            pltpu.VMEM((rows, dense), f32),
            pltpu.VMEM((rows, 128), f32),
            pltpu.VMEM((rows, 128), f32),
            pltpu.VMEM((rows, hidden), bf16),
            pltpu.VMEM((rows, dense), bf16),
            pltpu.VMEM((pieces, tp, ep, last, piece), bf16),
            pltpu.VMEM((pieces, ep, last, piece), bf16),
            pltpu.VMEM((pieces, ep, last, piece), bf16),
            pltpu.VMEM((pieces, ep, last, piece), bf16),
            dma((14,)),
            dma((batches,)),
            dma((10,)),
            *[dma((ep,))] * 10,
            dma,
            dma,
            *[dma((ep,))] * 4,
            dma((pieces,)),
            dma((pieces,)),
            dma((pieces, ep)),
            dma((pieces, ep)),
        ],
        compiler_params=pltpu.CompilerParams(
            collective_id=0, has_side_effects=True, vmem_limit_bytes=54 * 2**20
        ),
        name="layer",
    )(
        fresh_inputs,
        memory_arrays,
        chosen_specialist.T,
        chosen_coefficient.T,
        row(first_rescale),
        row(second_rescale),
        common_switch.reshape(-1, 128),
        instant_reward,
        row(lane_scaling),
        receiver_projector,
        address_projector,
        content_projector,
        final_projector,
        forget_narrowing.T,
        forget_widening,
        row(forget_bias),
        learning_narrowing.T,
        learning_widening,
        row(learning_bias),
        specialist_switch,
        specialist_expand,
        specialist_contract,
        common_activator.T,
        common_expand.T,
        common_contract,
    )
    return pl.pallas_call(
        settle_kernel,
        out_shape=(
            jax.ShapeDtypeStruct((last, width), bf16),
            jax.ShapeDtypeStruct(memory_arrays.shape, f32),
        ),
        in_specs=[vmem] * 2,
        out_specs=(hbm,) * 2,
        scratch_shapes=[dma((5,))],
        compiler_params=pltpu.CompilerParams(vmem_limit_bytes=2**20),
        name="settle",
    )(
        pltpu.with_memory_space_constraint(new_tokens, pltpu.VMEM),
        pltpu.with_memory_space_constraint(memory_after, pltpu.VMEM),
    )


def solution(mesh):
    placed = (
        P(("grp", "ep"), None),
        P(("grp", "ep"), "tp", None, None),
        P(("grp", "ep"), None),
        P(("grp", "ep"), None),
        P(),
        P(),
        P("tp", "ep"),
        P("tp", "ep"),
        P("tp", "ep"),
        P("tp", "ep"),
        P(),
        P(None, "tp"),
        P("tp"),
        P(),
        P(None, "tp"),
        P("tp"),
        P("tp"),
        P("tp", None),
        P(None, ("ep", "tp")),
        P(None, ("ep", "tp")),
        P(("ep", "tp"), None),
        P(None, ("ep", "tp")),
        P(None, ("ep", "tp")),
        P(("ep", "tp"), None),
        P(),
    )
    return jax.shard_map(
        layer,
        mesh=mesh,
        in_specs=placed,
        out_specs=(P(("grp", "ep", "tp"), None), P(("grp", "ep"), "tp", None, None)),
        check_vma=False,
    )
```

```python
import functools
import math

import jax
import jax.numpy as jnp
from jax import lax
from jax.experimental import pallas as pl
from jax.experimental.pallas import tpu as pltpu
from jax.sharding import PartitionSpec as P

LANE_WIDTH = 64
FF_E = 7168


RMS_EPS = 1e-06
GROUP_EPS = 0.00064
HIGHEST = lax.Precision.HIGHEST
MESH = pl.DeviceIdType.MESH
VMEM_ROOM = 52 * 2**20


def rms_norm(values, norm_gain):
    mean_sq = jnp.mean(values * values, axis=-1, keepdims=True)
    return values * lax.rsqrt(mean_sq + RMS_EPS) * norm_gain


def widen(rounded):
    return lax.optimization_barrier(rounded).astype(jnp.float32)


def evolve_memory(
    memory_arrays,
    receiver_lanes,
    address_lanes,
    content_lanes,
    forget_lanes,
    learning_lanes,
    lane_rescale,
    instant_reward,
):
    unit_key = address_lanes * lax.rsqrt(
        jnp.sum(address_lanes * address_lanes, axis=-1, keepdims=True) + 1.0
    )
    stepped_address = address_lanes * learning_lanes
    removal = jnp.einsum("bhvk,bhk->bhv", memory_arrays, unit_key, precision=HIGHEST)
    memory_after = (
        memory_arrays * forget_lanes[:, :, None, :]
        - removal[..., None] * (unit_key * learning_lanes)[:, :, None, :]
        + content_lanes[..., None] * stepped_address[:, :, None, :]
    )
    memory_retrieval = jnp.einsum("bhvk,bhk->bhv", memory_after, receiver_lanes, precision=HIGHEST)
    centred = memory_retrieval - jnp.mean(memory_retrieval, axis=-1, keepdims=True)
    unit_address = centred * lax.rsqrt(
        jnp.mean(centred * centred, axis=-1, keepdims=True) + GROUP_EPS
    )
    instant_extra = (
        jnp.sum(receiver_lanes * stepped_address * instant_reward, axis=-1, keepdims=True)
        * content_lanes
    )
    return (memory_after, unit_address * lane_rescale + instant_extra)


def swiglu(rows_in, gate_w, up_w):
    gate_val = jnp.dot(rows_in, gate_w, preferred_element_type=jnp.float32)
    up_val = jnp.dot(rows_in, up_w, preferred_element_type=jnp.float32)
    return (jax.nn.silu(gate_val) * up_val).astype(jnp.bfloat16)


def body(
    fresh_inputs,
    memory_arrays,
    chosen_specialist,
    chosen_coefficient,
    first_rescale,
    second_rescale,
    receiver_projector,
    address_projector,
    content_projector,
    final_projector,
    forget_narrowing,
    forget_widening,
    forget_bias,
    learning_narrowing,
    learning_widening,
    learning_bias,
    lane_scaling,
    instant_reward,
    specialist_switch,
    specialist_expand,
    specialist_contract,
    common_activator,
    common_expand,
    common_contract,
    common_switch,
):
    own_rows = fresh_inputs.shape[0]
    model_width = fresh_inputs.shape[1]
    tp_count = lax.axis_size("tp")
    tp_rank = lax.axis_index("tp")
    half_width = model_width // tp_count
    head_count = half_width // LANE_WIDTH
    residual = fresh_inputs.astype(jnp.float32)
    normed = rms_norm(residual, first_rescale).astype(jnp.bfloat16)
    normed_half = lax.dynamic_slice_in_dim(normed, tp_rank * half_width, half_width, 1)
    local_weights = jnp.stack((receiver_projector, address_projector, content_projector), axis=1)
    projected_rows = jnp.einsum(
        "rd,dkc->rkc",
        lax.all_gather(normed_half, "ep", axis=0, tiled=True),
        local_weights,
        preferred_element_type=jnp.float32,
    ).astype(jnp.bfloat16)
    partial_value = lax.all_to_all(projected_rows, "ep", split_axis=0, concat_axis=2, tiled=True)
    projected = lax.psum(widen(partial_value).astype(jnp.bfloat16), "tp")
    mine = lax.dynamic_slice_in_dim(projected, tp_rank * half_width, half_width, 2)

    def divide_lanes(channels):
        return channels.astype(jnp.float32).reshape(own_rows, head_count, LANE_WIDTH)

    decay_mid = jnp.tanh(
        jnp.dot(normed, forget_narrowing, preferred_element_type=jnp.float32)
    ).astype(jnp.bfloat16)
    decay_pre = forget_bias + jnp.dot(
        decay_mid, forget_widening, preferred_element_type=jnp.float32
    )
    decay_vals = jnp.exp(-jnp.exp(-jax.nn.softplus(-decay_pre) - 0.5))
    rate_mid = jnp.dot(normed, learning_narrowing, preferred_element_type=jnp.float32).astype(
        jnp.bfloat16
    )
    rate_vals = jax.nn.sigmoid(
        learning_bias + jnp.dot(rate_mid, learning_widening, preferred_element_type=jnp.float32)
    )
    memory_after, memory_retrieval = evolve_memory(
        memory_arrays,
        divide_lanes(mine[:, 0]),
        divide_lanes(mine[:, 1]),
        divide_lanes(mine[:, 2]),
        divide_lanes(decay_vals),
        divide_lanes(rate_vals),
        lane_scaling.reshape(head_count, LANE_WIDTH),
        instant_reward,
    )
    attended = memory_retrieval.reshape(own_rows, half_width).astype(jnp.bfloat16)
    done_rows = jnp.dot(
        lax.all_gather(attended, "ep", axis=0, tiled=True),
        final_projector,
        preferred_element_type=jnp.float32,
    ).astype(jnp.bfloat16)
    out_part = lax.all_to_all(done_rows, "ep", split_axis=0, concat_axis=1, tiled=True)
    mixed_out = lax.psum(widen(out_part).astype(jnp.bfloat16), "tp")
    residual = residual + mixed_out.astype(jnp.float32)
    ffn_in = rms_norm(residual, second_rescale).astype(jnp.bfloat16)
    all_in, all_weight, all_ids = (
        lax.all_gather(ffn_in, "ep", axis=0, tiled=True),
        lax.all_gather(chosen_coefficient, "ep", axis=0, tiled=True),
        lax.all_gather(chosen_specialist, "ep", axis=0, tiled=True),
    )
    column_count = specialist_switch.shape[1]
    flat_rank = lax.axis_index("ep") * tp_count + tp_rank
    expert = flat_rank * column_count // FF_E
    expert_share = jnp.sum(
        jnp.where(all_ids == expert, all_weight.astype(jnp.float32), 0.0), axis=1
    )
    hidden = swiglu(all_in, specialist_switch, specialist_expand)
    shared_hidden = swiglu(all_in, common_activator, common_expand)
    branch_scale = jax.nn.sigmoid(
        jnp.dot(all_in, common_switch, preferred_element_type=jnp.float32)
    )
    rows_mine = own_rows // tp_count
    expert_term = expert_share[:, None] * jnp.dot(
        hidden, specialist_contract, preferred_element_type=jnp.float32
    )
    routed = lax.psum_scatter(
        expert_term
        + branch_scale[:, None]
        * jnp.dot(shared_hidden, common_contract, preferred_element_type=jnp.float32),
        ("ep", "tp"),
        scatter_dimension=0,
        tiled=True,
    )
    own_residual = lax.dynamic_slice_in_dim(residual, tp_rank * rows_mine, rows_mine, 0)
    return ((own_residual + routed).astype(jnp.bfloat16), memory_after)


def flipped(index, mask, count):
    total, step = 0, 1
    while step < count:
        total = total + step * lax.rem(index // step + mask // step, 2)
        step = 2 * step
    return total


def _greet(ep, tp):
    me, core = lax.axis_index("ep"), lax.axis_index("tp")
    barrier = pltpu.get_barrier_semaphore()
    for mask in range(ep - 1, -1, -1):
        for side in range(tp):
            if mask or side:
                pl.semaphore_signal(
                    barrier,
                    inc=1,
                    device_id={"ep": flipped(me, mask, ep), "tp": lax.rem(core + side, tp)},
                    device_id_type=MESH,
                )


def _met(ep, tp):
    pl.semaphore_wait(pltpu.get_barrier_semaphore(), ep * tp - 1)


def _remote(src, dst, send, recv, e, t):
    return pltpu.make_async_remote_copy(
        src_ref=src,
        dst_ref=dst,
        send_sem=send,
        recv_sem=recv,
        device_id={"ep": e, "tp": t},
        device_id_type=MESH,
    )


def across_dot(left, right):
    return lax.dot_general(
        left, right, (((1,), (1,)), ((), ())), preferred_element_type=jnp.float32
    )


def arrive(ref, sem):
    pltpu.make_async_copy(ref, ref, sem).wait()


def layer_kernel(
    ep, tp, expert_cols,
    x_h, memory, ids_h, coef_h, gain_h, gain2_h, cs_h, reward_h, scaling_h,
    wq_h, wk_h, wv_h, wo_h, fnar_h, fwid_h, fbias_h, lnar_h, lwid_h, lbias_h,
    wg_h, wu_h, wd_h, cg_h, cu_h, cd_h,
    out, mem,
    x, ids, coef, gains, cs16, cs, reward, rows_in, narrow, widen_w,
    w, wo, wgu, wd, cgu, cd, pk, pk16,
    halves, rows_all, part, gotp, dch, rch, wch, same, pick,
    moves, factors, att, att_all, xcol, share, pbuf, psib, res,
    gacc, uacc, cgacc, cuacc, sq, gs, hid, chid, sibout, sibin, mine, got,
    lsem, msem, wsem,
    s_row, r_row, t_row, s_part, a_part, r_part, s_att, r_att, t_att, s_x, r_x, s_sh, r_sh,
    s_p, r_p, s_res, r_res, f_res, b_res, s_sib, r_sib, s_out, r_out,
):
    gain, gain2 = gains.at[0], gains.at[1]
    fbias, lbias, scaling = rows_in.at[0], rows_in.at[1], rows_in.at[2]
    wg, wu, cg, cu = wgu.at[0], wgu.at[1], cgu.at[0], cgu.at[1]
    me, core = lax.axis_index("ep"), lax.axis_index("tp")
    mate = lax.rem(core + 1, tp)
    group = ep // tp
    side = me // group
    own, width = x.shape
    half = width // tp
    cols = wo.shape[1]
    rows = ep * own
    heads = half // LANE_WIDTH
    pack = pk.shape[2] // LANE_WIDTH
    packs = heads // pack
    block_rows = packs * LANE_WIDTH
    far = list(range(1, ep))
    turn_at, turned_by = ep // 2, ep // 2 + 1
    direct = [turn_at] + [k for k in far if k not in (turn_at, turned_by)]
    _greet(ep, tp)

    def load(sem, *pairs):
        return [pltpu.make_async_copy(a, b, sem) for a, b in pairs]

    batches = 4
    batch = own // batches
    early = load(lsem.at[0], (x_h, x)) + load(lsem.at[1], (gain_h, gain), (gain2_h, gain2))
    smalls = (
        load(lsem.at[2], (fnar_h, narrow.at[0]), (lnar_h, narrow.at[1]))
        + load(lsem.at[3], (fwid_h, widen_w.at[0]), (lwid_h, widen_w.at[1]))
        + load(lsem.at[4], (fbias_h, fbias), (lbias_h, lbias), (scaling_h, scaling))
        + load(lsem.at[5], (reward_h, reward))
        + load(lsem.at[6], (ids_h, ids))
        + load(lsem.at[7], (coef_h, coef))
        + load(lsem.at[8], (cs_h, cs16))
        + load(wsem.at[0], (wq_h, w.at[0]), (wk_h, w.at[1]), (wv_h, w.at[2]))
    )
    states = [
        pltpu.make_async_copy(
            memory.at[pl.ds(i * batch, batch)], mem.at[pl.ds(i * batch, batch)], msem
        )
        for i in range(batches)
    ]
    weights = (
        load(wsem.at[1], (wo_h, wo))
        + load(wsem.at[2], (wg_h, wg), (wu_h, wu))
        + load(wsem.at[3], (cg_h, cg), (cu_h, cu))
        + load(wsem.at[4], (wd_h, wd))
        + load(wsem.at[5], (cd_h, cd))
    )
    for copy in early + smalls + states:
        copy.start()

    def push(*args):
        _remote(*args).start()

    def spread_out(block, every, send, recv, turn):
        for k in direct:
            arrives = turn if k == turn_at else recv
            push(block, every.at[me], send, arrives, flipped(me, k, ep), core)

    def hand_on(every, send, recv, turn):
        e = flipped(me, turn_at, ep)
        arrive(every.at[e], turn)
        push(every.at[e], every.at[e], send, recv, flipped(me, 1, ep), core)

    arrive(x, lsem.at[0])
    arrive(gains, lsem.at[1])
    normed = rms_norm(x[...].astype(jnp.float32), gain[...]).astype(jnp.bfloat16)
    for i in range(tp):
        halves[i] = normed[:, i * half : (i + 1) * half]
    _met(ep, tp)
    spread_out(halves.at[core], rows_all, s_row, r_row, t_row)
    rows_all[me] = halves[core]

    for ref, at in ((narrow, 2), (widen_w, 3), (rows_in, 4), (reward, 5), (ids, 6), (coef, 7), (cs16, 8)):
        arrive(ref, lsem.at[at])
    cs[...] = cs16[...].astype(jnp.float32)
    decay_mid = jnp.tanh(across_dot(normed, narrow[0])).astype(jnp.bfloat16)
    decay_pre = fbias[...] + jnp.dot(decay_mid, widen_w[0], preferred_element_type=jnp.float32)
    kept = jnp.exp(-(math.exp(-0.5) / (1.0 + jnp.exp(-decay_pre))))
    dch[...] = kept
    rate_mid = across_dot(normed, narrow[1]).astype(jnp.bfloat16)
    rate_pre = lbias[...] + jnp.dot(rate_mid, widen_w[1], preferred_element_type=jnp.float32)
    rch[...] = 1.0 / (1.0 + jnp.exp(-rate_pre))
    for h in range(heads):
        wch[:, h * LANE_WIDTH : (h + 1) * LANE_WIDTH] = reward[h : h + 1]
    first = lax.broadcasted_iota(jnp.int32, same.shape, 0) // LANE_WIDTH
    other = lax.broadcasted_iota(jnp.int32, same.shape, 1) // LANE_WIDTH
    same[...] = jnp.where(first == other, 1.0, 0.0).astype(jnp.bfloat16)
    line = lax.broadcasted_iota(jnp.int32, (own, pick.shape[2]), 0)
    for b in range(own):
        pick[b] = jnp.where(line == b, 1.0, 0.0).astype(jnp.bfloat16)
    lane = lax.broadcasted_iota(jnp.int32, (own, 128), 1)
    routes = jnp.zeros((own, 128), jnp.float32)
    ids_cols, coef_cols = ids[...].T, coef[...].astype(jnp.float32).T
    for i in range(ids.shape[0]):
        routes = routes + jnp.where(
            ids_cols[:, i : i + 1] == lane, coef_cols[:, i : i + 1], 0.0
        )
    share[me] = routes.astype(jnp.bfloat16)
    xcol[me] = x[:, pl.ds(pl.multiple_of(me * cols, cols), cols)]
    hand_on(rows_all, s_row, r_row, t_row)
    arrive(mem, msem)
    for copy in weights:
        copy.start()

    def join(b, _):
        for p in range(packs):
            joined = jnp.concatenate([mem[b, p * pack + i] for i in range(pack)], axis=-1)
            at = slice(p * LANE_WIDTH, (p + 1) * LANE_WIDTH)
            pk[b, at] = joined
            pk16[b, at] = joined.astype(jnp.bfloat16)
        return _

    lax.fori_loop(0, own, join, 0)

    arrive(w, wsem.at[0])
    arrive(rows_all.at[pl.ds(0, ep - 2)], r_row)
    every = rows_all[...].reshape(rows, half)
    for i in range(3):
        done = jnp.dot(every, w[i], preferred_element_type=jnp.float32)
        part[:, i] = done.astype(jnp.bfloat16).reshape(ep, own, cols)
    place = lax.rem(me, group)
    slot = core * group + place
    for k in far:
        e = flipped(me, k, ep)
        push(part.at[e], gotp.at[slot], s_part, r_part.at[place], e, side)
    here = side == core
    local = pltpu.make_async_copy(part.at[me], gotp.at[slot], r_part.at[place])
    across = _remote(part.at[me], gotp.at[slot], a_part, r_part.at[place], me, side)

    @pl.when(here)
    def _():
        local.start()

    @pl.when(jnp.logical_not(here))
    def _():
        across.start()

    blocks = []
    for k in far:
        e = flipped(me, k, ep)
        block = x.at[:, pl.ds(pl.multiple_of(e * cols, cols), cols)]
        blocks.append(_remote(block, xcol.at[me], s_x, r_x, e, core))

    @pl.when(here)
    def _():
        for copy in blocks:
            copy.start()

    for k in far:
        push(share.at[me], share.at[me], s_sh, r_sh, flipped(me, k, ep), core)

    wide = pack * LANE_WIDTH
    inner = lax.broadcasted_iota(jnp.int32, (own, wide), 1) // LANE_WIDTH

    def within(channels):
        high = channels.astype(jnp.bfloat16)
        low = (channels - high.astype(jnp.float32)).astype(jnp.bfloat16)
        both = jnp.dot(
            jnp.concatenate([high, low], axis=0), same[...], preferred_element_type=jnp.float32
        )
        return both[: channels.shape[0]] + both[channels.shape[0] :]

    def stack(*kinds):
        return jnp.concatenate(
            [jnp.where(inner == i, kind, 0.0) for kind in kinds for i in range(pack)], axis=0
        ).astype(jnp.bfloat16)

    def only(stacked, b):
        split = stacked.reshape(2 * pack, own, wide) * pick[b][None]
        return split.reshape(2 * pack * own, wide)

    def lanes_of(lines):
        return jnp.concatenate(
            [lines[i * own : (i + 1) * own] for i in range(pack)], axis=-1
        )

    def rows_of(channels):
        return jnp.concatenate(
            [channels[:, i * LANE_WIDTH : (i + 1) * LANE_WIDTH] for i in range(pack)], axis=0
        )

    def column_of(channels):
        return jnp.concatenate(
            [channels[:, i * LANE_WIDTH : i * LANE_WIDTH + 1] for i in range(pack)], axis=0
        )

    def pass_att(j):
        hand_on(att_all.at[j], s_att, r_att, t_att.at[j])

    order = [flipped(lax.rem(me, group), j, group) for j in range(packs)]
    for turn, j in enumerate(order):
        arrive(gotp.at[pl.ds(0, tp)], r_part.at[j])
        sums = []
        for i in range(3):
            total = gotp[j, i].astype(jnp.float32)
            for s in range(1, tp):
                total = total + gotp[s * group + j, i].astype(jnp.float32)
            sums.append(total.astype(jnp.bfloat16).astype(jnp.float32))
        q, k, v = sums
        at = pl.ds(pl.multiple_of(j * wide, wide), wide)
        down = pl.ds(pl.multiple_of(j * LANE_WIDTH, LANE_WIDTH), LANE_WIDTH)
        r = rch[:, at]
        scaled = k * r
        met = scaled * q
        sizes = within(jnp.concatenate([k * k, met, met * wch[:, at]], axis=0))
        inverse = lax.rsqrt(sizes[:own] + 1.0)
        unit = k * inverse
        stacked = stack(unit, dch[:, at] * q)
        v_rows = rows_of(v)
        acc = jnp.zeros((128, LANE_WIDTH), jnp.float32)
        for b in range(own):
            acc = acc + across_dot(only(stacked, b), pk16[b, down])
        key_met = sizes[own : 2 * own]
        seen = (
            acc[pack * own :]
            - acc[: pack * own] * column_of(inverse * key_met)
            + v_rows * column_of(key_met)
        )
        centred = seen - jnp.mean(seen, axis=-1, keepdims=True)
        level = lax.rsqrt(jnp.mean(centred * centred, axis=-1, keepdims=True) + GROUP_EPS)
        att[j] = (
            lanes_of(centred * level) * scaling[:, at] + sizes[2 * own :] * v
        ).astype(jnp.bfloat16)
        spread_out(att.at[j], att_all.at[j], s_att, r_att, t_att.at[j])
        att_all[j, me] = att[j]
        factors[j] = (
            jnp.concatenate([acc[: pack * own], v_rows], axis=0).T.astype(jnp.bfloat16)
        )
        moves[j] = stack(-(unit * r), scaled)
        if turn > 2:
            pass_att(order[turn - 3])
    def renew(b, _):
        for p in range(packs):
            change = jnp.dot(factors[p], only(moves[p], b), preferred_element_type=jnp.float32)
            at = slice(p * LANE_WIDTH, (p + 1) * LANE_WIDTH)
            new = pk[b, at] * dch[pl.ds(b, 1), p * wide : (p + 1) * wide] + change
            for i in range(pack):
                mem[b, p * pack + i] = new[:, i * LANE_WIDTH : (i + 1) * LANE_WIDTH]
        return _

    eighth = own // 8
    for turn in range(1, packs):
        lax.fori_loop((turn - 1) * eighth, turn * eighth, renew, 0)
        pass_att(order[turn])
    lax.fori_loop((packs - 1) * eighth, own // 2, renew, 0)
    arrive(wo, wsem.at[1])
    arrive(share.at[pl.ds(0, ep - 1)], r_sh)
    arrive(att_all.at[:, pl.ds(0, ep - 2)], r_att)
    done = jnp.zeros((rows, cols), jnp.float32)
    for j in range(packs):
        done = done + jnp.dot(
            att_all[j].reshape(rows, wide),
            wo[j * wide : (j + 1) * wide],
            preferred_element_type=jnp.float32,
        )
    done = done.astype(jnp.bfloat16)
    pbuf[...] = done.reshape(tp, group * own, cols)
    push(pbuf.at[mate], psib, s_p, r_p, me, mate)

    @pl.when(here)
    def _():
        arrive(xcol.at[pl.ds(0, group - 1)], r_x)

    @pl.when(jnp.logical_not(here))
    def _():
        arrive(xcol.at[pl.ds(0, group)], r_x)

    arrive(psib, r_p)
    mixed = (pbuf[core].astype(jnp.float32) + psib[...].astype(jnp.float32)).astype(jnp.bfloat16)
    held = xcol[pl.ds(core * group, group)].reshape(group * own, cols).astype(jnp.float32)
    res[me, core] = (held + mixed.astype(jnp.float32)).astype(jnp.bfloat16)
    for k in direct:
        push(res.at[me, core], res.at[me, core], s_res, r_res.at[me], flipped(me, k, ep), core)
    push(res.at[me, core], res.at[me, core], f_res, b_res.at[me], me, mate)
    for ref in (gacc, uacc, cgacc, cuacc, sq, gs):
        ref[...] = jnp.zeros_like(ref)
    arrive(wgu, wsem.at[2])
    arrive(cgu, wsem.at[3])

    def forward(e):
        push(res.at[e, core], res.at[e, core], f_res, b_res.at[e], me, mate)

    def absorb(e):
        arrive(res.at[e, mate], b_res.at[e])
        at = pl.ds(pl.multiple_of(e * cols, cols), cols)
        block = res[e].reshape(rows, cols).astype(jnp.float32)
        scaled = (block * gain2[:, at]).astype(jnp.bfloat16)
        gacc[...] += jnp.dot(scaled, wg[at, :], preferred_element_type=jnp.float32)
        uacc[...] += jnp.dot(scaled, wu[at, :], preferred_element_type=jnp.float32)
        cgacc[...] += across_dot(scaled, cg[:, at])
        cuacc[...] += across_dot(scaled, cu[:, at])
        wide_rows = scaled.astype(jnp.float32)
        for i in range(cols // 128):
            part_of = block[:, i * 128 : (i + 1) * 128]
            sq[...] += part_of * part_of
            line = cs[pl.ds(e * (cols // 128) + i, 1), :]
            gs[...] += wide_rows[:, i * 128 : (i + 1) * 128] * line

    ready = me
    for k in (1, 2, turn_at, *[k for k in range(3, ep) if k not in (turn_at, turned_by)], turned_by):
        e = flipped(me, k, ep)
        arrive(res.at[e, core], r_res.at[e])
        if k == turn_at:
            push(
                res.at[e, core], res.at[e, core], s_res, r_res.at[e],
                flipped(me, 1, ep), core,
            )
        forward(e)
        absorb(ready)
        ready = e
    absorb(ready)
    inv = lax.rsqrt(jnp.sum(sq[...], axis=-1, keepdims=True) / width + RMS_EPS)
    branch_scale = 1.0 / (1.0 + jnp.exp(-inv * jnp.sum(gs[...], axis=-1, keepdims=True)))
    expert = (me * tp + core) * wg.shape[1] // expert_cols
    table = share[...].astype(jnp.float32).reshape(rows, 128)
    picked = lax.broadcasted_iota(jnp.int32, (rows, 128), 1) == expert
    weight = jnp.sum(jnp.where(picked, table, 0.0), axis=-1, keepdims=True)

    def gated(target, gates, ups):
        g, u = gates[...] * inv, ups[...] * inv
        target[...] = (g / (1.0 + jnp.exp(-g)) * u).astype(jnp.bfloat16)

    gated(hid, gacc, uacc)
    gated(chid, cgacc, cuacc)
    arrive(wd, wsem.at[4])
    arrive(cd, wsem.at[5])
    pieces = mine.shape[0]
    piece = width // pieces
    last = own // tp

    def finish(n):
        arrive(sibin.at[n], r_sib.at[n])
        mine[n] = (
            sibout[n, core].astype(jnp.float32) + sibin[n].astype(jnp.float32)
        ).astype(jnp.bfloat16)
        for k in far:
            e = flipped(me, k, ep)
            push(mine.at[n, e], got.at[n, me], s_out, r_out.at[n], e, core)

    for n in range(pieces):
        at = slice(n * piece, (n + 1) * piece)
        y = weight * jnp.dot(hid[...], wd[:, at], preferred_element_type=jnp.float32)
        y = y + branch_scale * jnp.dot(chid[...], cd[:, at], preferred_element_type=jnp.float32)
        y = y.reshape(ep, tp, last, piece)
        for i in range(tp):
            sibout[n, i] = y[:, i].astype(jnp.bfloat16)
        push(sibout.at[n, mate], sibin.at[n], s_sib, r_sib.at[n], me, mate)
        if n:
            finish(n - 1)
    finish(pieces - 1)
    lax.fori_loop(own // 2, own, renew, 0)
    start = pl.multiple_of(lax.rem(me, group) * own, own)
    per = piece // cols
    for n in range(pieces):
        arrive(got.at[n, pl.ds(0, ep - 1)], r_out.at[n])
        total = mine[n, me].astype(jnp.float32)
        for k in far:
            total = total + got[n, flipped(me, k, ep)].astype(jnp.float32)
        for s in range(per):
            base = res[n * per + s, side, pl.ds(start, own)].astype(jnp.float32)
            base = jnp.where(core == 0, base[:last], base[last:])
            a = n * piece + s * cols
            out[:, a : a + cols] = (base + total[:, s * cols : (s + 1) * cols]).astype(jnp.bfloat16)
    arrive(rows_all.at[pl.ds(0, ep - 1)], s_row)
    arrive(part.at[pl.ds(0, ep - 1)], s_part)
    arrive(att_all.at[:, pl.ds(0, ep - 1)], s_att)
    arrive(share.at[pl.ds(0, ep - 1)], s_sh)
    arrive(psib, s_p)
    arrive(res.at[pl.ds(0, ep - 1), 0], s_res)
    arrive(res.at[:, 0], f_res)
    arrive(sibin, s_sib)
    arrive(got.at[:, pl.ds(0, ep - 1)], s_out)

    @pl.when(jnp.logical_not(here))
    def _():
        across.wait_send()

    @pl.when(here)
    def _():
        arrive(xcol.at[pl.ds(0, ep - 1)], s_x)


def settle_kernel(tokens, state, out, after, sems):
    step = state.shape[0] // (sems.shape[0] - 1)
    copies = [pltpu.make_async_copy(tokens, out, sems.at[0])]
    for i in range(sems.shape[0] - 1):
        at = pl.ds(i * step, step)
        copies.append(pltpu.make_async_copy(state.at[at], after.at[at], sems.at[i + 1]))
    for copy in copies:
        copy.start()
    for copy in copies:
        copy.wait()


def layer(*blocks):
    own = blocks[0].shape[0]
    cols, hidden = blocks[9].shape[1], blocks[18].shape[1]
    heads = blocks[17].shape[0]
    tiles = cols % 128 == 0 and hidden % 256 == 0 and own % 16 == 0
    tiles = tiles and heads % 8 == 0 and 128 % heads == 0 and heads <= 32
    tiles = tiles and blocks[0].shape[1] % 2048 == 0 and cols == 4 * LANE_WIDTH and own == 16
    ep = lax.axis_size("ep")
    heads_match = ep in (4, 8) and lax.axis_size("tp") == 2
    weights = sum(2 * w.size for w in blocks[18:24])
    rows = own * ep
    held = weights + rows * (12 * blocks[0].shape[1] + 8 * hidden) + 14 * blocks[1].size
    small = held < VMEM_ROOM
    return (kernel_body if tiles and heads_match and small else body)(*blocks)


def kernel_body(
    fresh_inputs,
    memory_arrays,
    chosen_specialist,
    chosen_coefficient,
    first_rescale,
    second_rescale,
    receiver_projector,
    address_projector,
    content_projector,
    final_projector,
    forget_narrowing,
    forget_widening,
    forget_bias,
    learning_narrowing,
    learning_widening,
    learning_bias,
    lane_scaling,
    instant_reward,
    specialist_switch,
    specialist_expand,
    specialist_contract,
    common_activator,
    common_expand,
    common_contract,
    common_switch,
):
    ep, tp = lax.axis_size("ep"), lax.axis_size("tp")
    own, width = fresh_inputs.shape
    half, cols = width // tp, final_projector.shape[1]
    heads = half // LANE_WIDTH
    group = ep // tp
    vmem = pl.BlockSpec(memory_space=pltpu.VMEM)
    hbm = pl.BlockSpec(memory_space=pl.ANY)
    bf16, f32 = jnp.bfloat16, jnp.float32
    dma = pltpu.SemaphoreType.DMA

    def row(vector):
        return vector.reshape(1, -1)

    rows, hidden, dense = ep * own, specialist_switch.shape[1], common_activator.shape[1]
    low, top = forget_narrowing.shape[1], chosen_specialist.shape[1]
    pack = 4
    wide, block_rows = pack * LANE_WIDTH, heads // pack * LANE_WIDTH
    pieces = 4
    piece, last = width // pieces, own // tp
    new_tokens, memory_after = pl.pallas_call(
        functools.partial(layer_kernel, ep, tp, FF_E),
        out_shape=(
            pltpu.VMEM((last, width), bf16),
            pltpu.VMEM(memory_arrays.shape, f32),
        ),
        in_specs=[hbm] * 25,
        out_specs=(vmem, vmem),
        scratch_shapes=[
            pltpu.VMEM((own, width), bf16),
            pltpu.VMEM((top, own), jnp.int32),
            pltpu.VMEM((top, own), bf16),
            pltpu.VMEM((2, 1, width), f32),
            pltpu.VMEM((width // 128, 128), bf16),
            pltpu.VMEM((width // 128, 128), f32),
            pltpu.VMEM((heads, LANE_WIDTH), f32),
            pltpu.VMEM((3, 1, half), f32),
            pltpu.VMEM((2, low, width), bf16),
            pltpu.VMEM((2, low, half), bf16),
            pltpu.VMEM((3, half, cols), bf16),
            pltpu.VMEM((half, cols), bf16),
            pltpu.VMEM((2, width, hidden), bf16),
            pltpu.VMEM((hidden, width), bf16),
            pltpu.VMEM((2, dense, width), bf16),
            pltpu.VMEM((dense, width), bf16),
            pltpu.VMEM((own, block_rows, wide), f32),
            pltpu.VMEM((own, block_rows, wide), bf16),
            pltpu.VMEM((tp, own, half), bf16),
            pltpu.VMEM((ep, own, half), bf16),
            pltpu.VMEM((ep, 3, own, cols), bf16),
            pltpu.VMEM((ep, 3, own, cols), bf16),
            pltpu.VMEM((own, half), f32),
            pltpu.VMEM((own, half), f32),
            pltpu.VMEM((1, half), f32),
            pltpu.VMEM((wide, wide), bf16),
            pltpu.VMEM((own, own, wide), bf16),
            pltpu.VMEM((heads // pack, 128, wide), bf16),
            pltpu.VMEM((heads // pack, LANE_WIDTH, 128), bf16),
            pltpu.VMEM((heads // pack, own, wide), bf16),
            pltpu.VMEM((heads // pack, ep, own, wide), bf16),
            pltpu.VMEM((ep, own, cols), bf16),
            pltpu.VMEM((ep, own, 128), bf16),
            pltpu.VMEM((tp, group * own, cols), bf16),
            pltpu.VMEM((group * own, cols), bf16),
            pltpu.VMEM((ep, tp, group * own, cols), bf16),
            pltpu.VMEM((rows, hidden), f32),
            pltpu.VMEM((rows, hidden), f32),
            pltpu.VMEM((rows, dense), f32),
            pltpu.VMEM((rows, dense), f32),
            pltpu.VMEM((rows, 128), f32),
            pltpu.VMEM((rows, 128), f32),
            pltpu.VMEM((rows, hidden), bf16),
            pltpu.VMEM((rows, dense), bf16),
            pltpu.VMEM((pieces, tp, ep, last, piece), bf16),
            pltpu.VMEM((pieces, ep, last, piece), bf16),
            pltpu.VMEM((pieces, ep, last, piece), bf16),
            pltpu.VMEM((pieces, ep, last, piece), bf16),
            dma((9,)),
            dma,
            dma((6,)),
            *[dma] * 5,
            dma((group,)),
            *[dma] * 2,
            dma((heads // pack,)),
            *[dma] * 7,
            dma((ep,)),
            dma,
            dma((ep,)),
            dma,
            dma((pieces,)),
            dma,
            dma((pieces,)),
        ],
        compiler_params=pltpu.CompilerParams(
            collective_id=0, has_side_effects=True, vmem_limit_bytes=54 * 2**20
        ),
        name="layer",
    )(
        fresh_inputs,
        memory_arrays,
        chosen_specialist.T,
        chosen_coefficient.T,
        row(first_rescale),
        row(second_rescale),
        common_switch.reshape(-1, 128),
        instant_reward,
        row(lane_scaling),
        receiver_projector,
        address_projector,
        content_projector,
        final_projector,
        forget_narrowing.T,
        forget_widening,
        row(forget_bias),
        learning_narrowing.T,
        learning_widening,
        row(learning_bias),
        specialist_switch,
        specialist_expand,
        specialist_contract,
        common_activator.T,
        common_expand.T,
        common_contract,
    )
    return pl.pallas_call(
        settle_kernel,
        out_shape=(
            jax.ShapeDtypeStruct((last, width), bf16),
            jax.ShapeDtypeStruct(memory_arrays.shape, f32),
        ),
        in_specs=[vmem] * 2,
        out_specs=(hbm,) * 2,
        scratch_shapes=[dma((5,))],
        compiler_params=pltpu.CompilerParams(vmem_limit_bytes=2**20),
        name="settle",
    )(
        pltpu.with_memory_space_constraint(new_tokens, pltpu.VMEM),
        pltpu.with_memory_space_constraint(memory_after, pltpu.VMEM),
    )


def solution(mesh):
    placed = (
        P(("grp", "ep"), None),
        P(("grp", "ep"), "tp", None, None),
        P(("grp", "ep"), None),
        P(("grp", "ep"), None),
        P(),
        P(),
        P("tp", "ep"),
        P("tp", "ep"),
        P("tp", "ep"),
        P("tp", "ep"),
        P(),
        P(None, "tp"),
        P("tp"),
        P(),
        P(None, "tp"),
        P("tp"),
        P("tp"),
        P("tp", None),
        P(None, ("ep", "tp")),
        P(None, ("ep", "tp")),
        P(("ep", "tp"), None),
        P(None, ("ep", "tp")),
        P(None, ("ep", "tp")),
        P(("ep", "tp"), None),
        P(),
    )
    return jax.shard_map(
        layer,
        mesh=mesh,
        in_specs=placed,
        out_specs=(P(("grp", "ep", "tp"), None), P(("grp", "ep"), "tp", None, None)),
        check_vma=False,
    )
```

```python
import functools
import math

import jax
import jax.numpy as jnp
from jax import lax
from jax.experimental import pallas as pl
from jax.experimental.pallas import tpu as pltpu
from jax.sharding import PartitionSpec as P

LANE_WIDTH = 64
FF_E = 7168


RMS_EPS = 1e-06
GROUP_EPS = 0.00064
HIGHEST = lax.Precision.HIGHEST
MESH = pl.DeviceIdType.MESH
VMEM_ROOM = 52 * 2**20


def rms_norm(values, norm_gain):
    mean_sq = jnp.mean(values * values, axis=-1, keepdims=True)
    return values * lax.rsqrt(mean_sq + RMS_EPS) * norm_gain


def widen(rounded):
    return lax.optimization_barrier(rounded).astype(jnp.float32)


def evolve_memory(
    memory_arrays,
    receiver_lanes,
    address_lanes,
    content_lanes,
    forget_lanes,
    learning_lanes,
    lane_rescale,
    instant_reward,
):
    unit_key = address_lanes * lax.rsqrt(
        jnp.sum(address_lanes * address_lanes, axis=-1, keepdims=True) + 1.0
    )
    stepped_address = address_lanes * learning_lanes
    removal = jnp.einsum("bhvk,bhk->bhv", memory_arrays, unit_key, precision=HIGHEST)
    memory_after = (
        memory_arrays * forget_lanes[:, :, None, :]
        - removal[..., None] * (unit_key * learning_lanes)[:, :, None, :]
        + content_lanes[..., None] * stepped_address[:, :, None, :]
    )
    memory_retrieval = jnp.einsum("bhvk,bhk->bhv", memory_after, receiver_lanes, precision=HIGHEST)
    centred = memory_retrieval - jnp.mean(memory_retrieval, axis=-1, keepdims=True)
    unit_address = centred * lax.rsqrt(
        jnp.mean(centred * centred, axis=-1, keepdims=True) + GROUP_EPS
    )
    instant_extra = (
        jnp.sum(receiver_lanes * stepped_address * instant_reward, axis=-1, keepdims=True)
        * content_lanes
    )
    return (memory_after, unit_address * lane_rescale + instant_extra)


def swiglu(rows_in, gate_w, up_w):
    gate_val = jnp.dot(rows_in, gate_w, preferred_element_type=jnp.float32)
    up_val = jnp.dot(rows_in, up_w, preferred_element_type=jnp.float32)
    return (jax.nn.silu(gate_val) * up_val).astype(jnp.bfloat16)


def body(
    fresh_inputs,
    memory_arrays,
    chosen_specialist,
    chosen_coefficient,
    first_rescale,
    second_rescale,
    receiver_projector,
    address_projector,
    content_projector,
    final_projector,
    forget_narrowing,
    forget_widening,
    forget_bias,
    learning_narrowing,
    learning_widening,
    learning_bias,
    lane_scaling,
    instant_reward,
    specialist_switch,
    specialist_expand,
    specialist_contract,
    common_activator,
    common_expand,
    common_contract,
    common_switch,
):
    own_rows = fresh_inputs.shape[0]
    model_width = fresh_inputs.shape[1]
    tp_count = lax.axis_size("tp")
    tp_rank = lax.axis_index("tp")
    half_width = model_width // tp_count
    head_count = half_width // LANE_WIDTH
    residual = fresh_inputs.astype(jnp.float32)
    normed = rms_norm(residual, first_rescale).astype(jnp.bfloat16)
    normed_half = lax.dynamic_slice_in_dim(normed, tp_rank * half_width, half_width, 1)
    local_weights = jnp.stack((receiver_projector, address_projector, content_projector), axis=1)
    projected_rows = jnp.einsum(
        "rd,dkc->rkc",
        lax.all_gather(normed_half, "ep", axis=0, tiled=True),
        local_weights,
        preferred_element_type=jnp.float32,
    ).astype(jnp.bfloat16)
    partial_value = lax.all_to_all(projected_rows, "ep", split_axis=0, concat_axis=2, tiled=True)
    projected = lax.psum(widen(partial_value).astype(jnp.bfloat16), "tp")
    mine = lax.dynamic_slice_in_dim(projected, tp_rank * half_width, half_width, 2)

    def divide_lanes(channels):
        return channels.astype(jnp.float32).reshape(own_rows, head_count, LANE_WIDTH)

    decay_mid = jnp.tanh(
        jnp.dot(normed, forget_narrowing, preferred_element_type=jnp.float32)
    ).astype(jnp.bfloat16)
    decay_pre = forget_bias + jnp.dot(
        decay_mid, forget_widening, preferred_element_type=jnp.float32
    )
    decay_vals = jnp.exp(-jnp.exp(-jax.nn.softplus(-decay_pre) - 0.5))
    rate_mid = jnp.dot(normed, learning_narrowing, preferred_element_type=jnp.float32).astype(
        jnp.bfloat16
    )
    rate_vals = jax.nn.sigmoid(
        learning_bias + jnp.dot(rate_mid, learning_widening, preferred_element_type=jnp.float32)
    )
    memory_after, memory_retrieval = evolve_memory(
        memory_arrays,
        divide_lanes(mine[:, 0]),
        divide_lanes(mine[:, 1]),
        divide_lanes(mine[:, 2]),
        divide_lanes(decay_vals),
        divide_lanes(rate_vals),
        lane_scaling.reshape(head_count, LANE_WIDTH),
        instant_reward,
    )
    attended = memory_retrieval.reshape(own_rows, half_width).astype(jnp.bfloat16)
    done_rows = jnp.dot(
        lax.all_gather(attended, "ep", axis=0, tiled=True),
        final_projector,
        preferred_element_type=jnp.float32,
    ).astype(jnp.bfloat16)
    out_part = lax.all_to_all(done_rows, "ep", split_axis=0, concat_axis=1, tiled=True)
    mixed_out = lax.psum(widen(out_part).astype(jnp.bfloat16), "tp")
    residual = residual + mixed_out.astype(jnp.float32)
    ffn_in = rms_norm(residual, second_rescale).astype(jnp.bfloat16)
    all_in, all_weight, all_ids = (
        lax.all_gather(ffn_in, "ep", axis=0, tiled=True),
        lax.all_gather(chosen_coefficient, "ep", axis=0, tiled=True),
        lax.all_gather(chosen_specialist, "ep", axis=0, tiled=True),
    )
    column_count = specialist_switch.shape[1]
    flat_rank = lax.axis_index("ep") * tp_count + tp_rank
    expert = flat_rank * column_count // FF_E
    expert_share = jnp.sum(
        jnp.where(all_ids == expert, all_weight.astype(jnp.float32), 0.0), axis=1
    )
    hidden = swiglu(all_in, specialist_switch, specialist_expand)
    shared_hidden = swiglu(all_in, common_activator, common_expand)
    branch_scale = jax.nn.sigmoid(
        jnp.dot(all_in, common_switch, preferred_element_type=jnp.float32)
    )
    rows_mine = own_rows // tp_count
    expert_term = expert_share[:, None] * jnp.dot(
        hidden, specialist_contract, preferred_element_type=jnp.float32
    )
    routed = lax.psum_scatter(
        expert_term
        + branch_scale[:, None]
        * jnp.dot(shared_hidden, common_contract, preferred_element_type=jnp.float32),
        ("ep", "tp"),
        scatter_dimension=0,
        tiled=True,
    )
    own_residual = lax.dynamic_slice_in_dim(residual, tp_rank * rows_mine, rows_mine, 0)
    return ((own_residual + routed).astype(jnp.bfloat16), memory_after)


def flipped(index, mask, count):
    total, step = 0, 1
    while step < count:
        total = total + step * lax.rem(index // step + mask // step, 2)
        step = 2 * step
    return total


def _greet(ep, tp):
    me, core = lax.axis_index("ep"), lax.axis_index("tp")
    barrier = pltpu.get_barrier_semaphore()
    for mask in range(ep - 1, -1, -1):
        for side in range(tp):
            if mask or side:
                pl.semaphore_signal(
                    barrier,
                    inc=1,
                    device_id={"ep": flipped(me, mask, ep), "tp": lax.rem(core + side, tp)},
                    device_id_type=MESH,
                )


def _met(ep, tp):
    pl.semaphore_wait(pltpu.get_barrier_semaphore(), ep * tp - 1)


def _remote(src, dst, send, recv, e, t):
    return pltpu.make_async_remote_copy(
        src_ref=src,
        dst_ref=dst,
        send_sem=send,
        recv_sem=recv,
        device_id={"ep": e, "tp": t},
        device_id_type=MESH,
    )


def across_dot(left, right):
    return lax.dot_general(
        left, right, (((1,), (1,)), ((), ())), preferred_element_type=jnp.float32
    )


def arrive(ref, sem):
    pltpu.make_async_copy(ref, ref, sem).wait()


def layer_kernel(
    ep, tp, expert_cols,
    x_h, memory, ids_h, coef_h, gain_h, gain2_h, cs_h, reward_h, scaling_h,
    wq_h, wk_h, wv_h, wo_h, fnar_h, fwid_h, fbias_h, lnar_h, lwid_h, lbias_h,
    wg_h, wu_h, wd_h, cg_h, cu_h, cd_h,
    out, mem,
    x, ids, coef, gains, cs16, cs, reward, rows_in, narrow, widen_w,
    w, wo, wgu, wd, cgu, cd, pk, pk16,
    halves, rows_all, part, gotp, dch, rch, wch, same, pick,
    moves, factors, att, att_all, xcol, share, pbuf, psib, res,
    gacc, uacc, cgacc, cuacc, sq, gs, hid, chid, sibout, sibin, mine, got,
    lsem, msem, wsem,
    s_row, r_row, t_row, s_part, a_part, r_part, s_att, r_att, t_att, s_x, r_x, s_sh, r_sh,
    s_p, r_p, s_res, r_res, f_res, b_res, s_sib, r_sib, s_out, r_out,
):
    gain, gain2 = gains.at[0], gains.at[1]
    fbias, lbias, scaling = rows_in.at[0], rows_in.at[1], rows_in.at[2]
    wg, wu, cg, cu = wgu.at[0], wgu.at[1], cgu.at[0], cgu.at[1]
    me, core = lax.axis_index("ep"), lax.axis_index("tp")
    mate = lax.rem(core + 1, tp)
    group = ep // tp
    side = me // group
    own, width = x.shape
    half = width // tp
    cols = wo.shape[1]
    rows = ep * own
    heads = half // LANE_WIDTH
    pack = pk.shape[2] // LANE_WIDTH
    packs = heads // pack
    block_rows = packs * LANE_WIDTH
    far = list(range(1, ep))
    turn_at, turned_by = ep // 2, ep // 2 + 1
    direct = [turn_at] + [k for k in far if k not in (turn_at, turned_by)]
    _greet(ep, tp)

    def load(sem, *pairs):
        return [pltpu.make_async_copy(a, b, sem) for a, b in pairs]

    batches = 4
    batch = own // batches
    early = load(lsem.at[0], (x_h, x)) + load(lsem.at[1], (gain_h, gain), (gain2_h, gain2))
    smalls = (
        load(lsem.at[2], (fnar_h, narrow.at[0]), (lnar_h, narrow.at[1]))
        + load(lsem.at[3], (fwid_h, widen_w.at[0]), (lwid_h, widen_w.at[1]))
        + load(lsem.at[4], (fbias_h, fbias), (lbias_h, lbias), (scaling_h, scaling))
        + load(lsem.at[5], (reward_h, reward))
        + load(lsem.at[6], (ids_h, ids))
        + load(lsem.at[7], (coef_h, coef))
        + load(lsem.at[8], (cs_h, cs16))
        + load(wsem.at[0], (wq_h, w.at[0]), (wk_h, w.at[1]), (wv_h, w.at[2]))
    )
    states = [
        pltpu.make_async_copy(
            memory.at[pl.ds(i * batch, batch)], mem.at[pl.ds(i * batch, batch)], msem
        )
        for i in range(batches)
    ]
    weights = (
        load(wsem.at[1], (wo_h, wo))
        + load(wsem.at[2], (wg_h, wg), (wu_h, wu))
        + load(wsem.at[3], (cg_h, cg), (cu_h, cu))
        + load(wsem.at[4], (wd_h, wd))
        + load(wsem.at[5], (cd_h, cd))
    )
    for copy in early + smalls + states:
        copy.start()

    def push(*args):
        _remote(*args).start()

    def spread_out(block, every, send, recv, turn):
        for k in direct:
            arrives = turn if k == turn_at else recv
            push(block, every.at[me], send, arrives, flipped(me, k, ep), core)

    def hand_on(every, send, recv, turn):
        e = flipped(me, turn_at, ep)
        arrive(every.at[e], turn)
        push(every.at[e], every.at[e], send, recv, flipped(me, 1, ep), core)

    arrive(x, lsem.at[0])
    arrive(gains, lsem.at[1])
    normed = rms_norm(x[...].astype(jnp.float32), gain[...]).astype(jnp.bfloat16)
    for i in range(tp):
        halves[i] = normed[:, i * half : (i + 1) * half]
    _met(ep, tp)
    spread_out(halves.at[core], rows_all, s_row, r_row, t_row)
    rows_all[me] = halves[core]

    for ref, at in ((narrow, 2), (widen_w, 3), (rows_in, 4), (reward, 5), (ids, 6), (coef, 7), (cs16, 8)):
        arrive(ref, lsem.at[at])
    cs[...] = cs16[...].astype(jnp.float32)
    decay_mid = jnp.tanh(across_dot(normed, narrow[0])).astype(jnp.bfloat16)
    decay_pre = fbias[...] + jnp.dot(decay_mid, widen_w[0], preferred_element_type=jnp.float32)
    kept = jnp.exp(-(math.exp(-0.5) / (1.0 + jnp.exp(-decay_pre))))
    dch[...] = kept
    rate_mid = across_dot(normed, narrow[1]).astype(jnp.bfloat16)
    rate_pre = lbias[...] + jnp.dot(rate_mid, widen_w[1], preferred_element_type=jnp.float32)
    rch[...] = 1.0 / (1.0 + jnp.exp(-rate_pre))
    for h in range(heads):
        wch[:, h * LANE_WIDTH : (h + 1) * LANE_WIDTH] = reward[h : h + 1]
    first = lax.broadcasted_iota(jnp.int32, same.shape, 0) // LANE_WIDTH
    other = lax.broadcasted_iota(jnp.int32, same.shape, 1) // LANE_WIDTH
    same[...] = jnp.where(first == other, 1.0, 0.0).astype(jnp.bfloat16)
    line = lax.broadcasted_iota(jnp.int32, (own, pick.shape[2]), 0)
    for b in range(own):
        pick[b] = jnp.where(line == b, 1.0, 0.0).astype(jnp.bfloat16)
    lane = lax.broadcasted_iota(jnp.int32, (own, 128), 1)
    routes = jnp.zeros((own, 128), jnp.float32)
    ids_cols, coef_cols = ids[...].T, coef[...].astype(jnp.float32).T
    for i in range(ids.shape[0]):
        routes = routes + jnp.where(
            ids_cols[:, i : i + 1] == lane, coef_cols[:, i : i + 1], 0.0
        )
    share[me] = routes.astype(jnp.bfloat16)
    xcol[me] = x[:, pl.ds(pl.multiple_of(me * cols, cols), cols)]
    arrive(mem, msem)
    for copy in weights:
        copy.start()

    def join(b, _):
        for p in range(packs):
            joined = jnp.concatenate([mem[b, p * pack + i] for i in range(pack)], axis=-1)
            at = slice(p * LANE_WIDTH, (p + 1) * LANE_WIDTH)
            pk[b, at] = joined
            pk16[b, at] = joined.astype(jnp.bfloat16)
        return _

    lax.fori_loop(0, own // 2, join, 0)
    hand_on(rows_all, s_row, r_row, t_row)
    lax.fori_loop(own // 2, own, join, 0)

    arrive(w, wsem.at[0])
    arrive(rows_all.at[pl.ds(0, ep - 2)], r_row)
    every = rows_all[...].reshape(rows, half)
    for i in range(3):
        done = jnp.dot(every, w[i], preferred_element_type=jnp.float32)
        part[:, i] = done.astype(jnp.bfloat16).reshape(ep, own, cols)
    place = lax.rem(me, group)
    slot = core * group + place
    for k in far:
        e = flipped(me, k, ep)
        push(part.at[e], gotp.at[slot], s_part, r_part.at[place], e, side)
    here = side == core
    local = pltpu.make_async_copy(part.at[me], gotp.at[slot], r_part.at[place])
    across = _remote(part.at[me], gotp.at[slot], a_part, r_part.at[place], me, side)

    @pl.when(here)
    def _():
        local.start()

    @pl.when(jnp.logical_not(here))
    def _():
        across.start()

    blocks = []
    for k in far:
        e = flipped(me, k, ep)
        block = x.at[:, pl.ds(pl.multiple_of(e * cols, cols), cols)]
        blocks.append(_remote(block, xcol.at[me], s_x, r_x, e, core))

    @pl.when(here)
    def _():
        for copy in blocks:
            copy.start()

    for k in far:
        push(share.at[me], share.at[me], s_sh, r_sh, flipped(me, k, ep), core)

    wide = pack * LANE_WIDTH
    inner = lax.broadcasted_iota(jnp.int32, (own, wide), 1) // LANE_WIDTH

    def within(channels):
        high = channels.astype(jnp.bfloat16)
        low = (channels - high.astype(jnp.float32)).astype(jnp.bfloat16)
        both = jnp.dot(
            jnp.concatenate([high, low], axis=0), same[...], preferred_element_type=jnp.float32
        )
        return both[: channels.shape[0]] + both[channels.shape[0] :]

    def stack(*kinds):
        return jnp.concatenate(
            [jnp.where(inner == i, kind, 0.0) for kind in kinds for i in range(pack)], axis=0
        ).astype(jnp.bfloat16)

    def only(stacked, b):
        split = stacked.reshape(2 * pack, own, wide) * pick[b][None]
        return split.reshape(2 * pack * own, wide)

    def lanes_of(lines):
        return jnp.concatenate(
            [lines[i * own : (i + 1) * own] for i in range(pack)], axis=-1
        )

    def rows_of(channels):
        return jnp.concatenate(
            [channels[:, i * LANE_WIDTH : (i + 1) * LANE_WIDTH] for i in range(pack)], axis=0
        )

    def column_of(channels):
        return jnp.concatenate(
            [channels[:, i * LANE_WIDTH : i * LANE_WIDTH + 1] for i in range(pack)], axis=0
        )

    def pass_att(j):
        hand_on(att_all.at[j], s_att, r_att, t_att.at[j])

    order = [flipped(lax.rem(me, group), j, group) for j in range(packs)]
    def channels_of(j):
        return pl.ds(pl.multiple_of(j * wide, wide), wide)

    def read_out(j):
        sums = []
        for i in range(3):
            total = gotp[j, i].astype(jnp.float32)
            for s in range(1, tp):
                total = total + gotp[s * group + j, i].astype(jnp.float32)
            sums.append(total.astype(jnp.bfloat16).astype(jnp.float32))
        q, k, v = sums
        at = channels_of(j)
        down = pl.ds(pl.multiple_of(j * LANE_WIDTH, LANE_WIDTH), LANE_WIDTH)
        scaled = k * rch[:, at]
        met = scaled * q
        sizes = within(jnp.concatenate([k * k, met, met * wch[:, at]], axis=0))
        inverse = lax.rsqrt(sizes[:own] + 1.0)
        unit = k * inverse
        stacked = stack(unit, dch[:, at] * q)
        v_rows = rows_of(v)
        acc = jnp.zeros((128, LANE_WIDTH), jnp.float32)
        for b in range(own):
            acc = acc + across_dot(only(stacked, b), pk16[b, down])
        key_met = sizes[own : 2 * own]
        seen = (
            acc[pack * own :]
            - acc[: pack * own] * column_of(inverse * key_met)
            + v_rows * column_of(key_met)
        )
        centred = seen - jnp.mean(seen, axis=-1, keepdims=True)
        level = lax.rsqrt(jnp.mean(centred * centred, axis=-1, keepdims=True) + GROUP_EPS)
        att[j] = (
            lanes_of(centred * level) * scaling[:, at] + sizes[2 * own :] * v
        ).astype(jnp.bfloat16)
        return acc, v_rows, unit, scaled

    def note(j, acc, v_rows, unit, scaled):
        att_all[j, me] = att[j]
        factors[j] = (
            jnp.concatenate([acc[: pack * own], v_rows], axis=0).T.astype(jnp.bfloat16)
        )
        moves[j] = stack(-(unit * rch[:, channels_of(j)]), scaled)

    for some in (order[:2], order[2:]):
        for j in some:
            arrive(gotp.at[pl.ds(0, tp)], r_part.at[j])
        kept = [read_out(j) for j in some]
        for j in some:
            spread_out(att.at[j], att_all.at[j], s_att, r_att, t_att.at[j])
        for j, parts in zip(some, kept):
            note(j, *parts)
    pass_att(order[0])
    def renew(b, _):
        for p in range(packs):
            change = jnp.dot(factors[p], only(moves[p], b), preferred_element_type=jnp.float32)
            at = slice(p * LANE_WIDTH, (p + 1) * LANE_WIDTH)
            new = pk[b, at] * dch[pl.ds(b, 1), p * wide : (p + 1) * wide] + change
            for i in range(pack):
                mem[b, p * pack + i] = new[:, i * LANE_WIDTH : (i + 1) * LANE_WIDTH]
        return _

    eighth = own // 8
    for turn in range(1, packs):
        lax.fori_loop((turn - 1) * eighth, turn * eighth, renew, 0)
        pass_att(order[turn])
    lax.fori_loop((packs - 1) * eighth, own // 2, renew, 0)
    arrive(wo, wsem.at[1])
    arrive(share.at[pl.ds(0, ep - 1)], r_sh)
    arrive(att_all.at[:, pl.ds(0, ep - 2)], r_att)
    done = jnp.zeros((rows, cols), jnp.float32)
    for j in range(packs):
        done = done + jnp.dot(
            att_all[j].reshape(rows, wide),
            wo[j * wide : (j + 1) * wide],
            preferred_element_type=jnp.float32,
        )
    done = done.astype(jnp.bfloat16)
    pbuf[...] = done.reshape(tp, group * own, cols)
    push(pbuf.at[mate], psib, s_p, r_p, me, mate)

    @pl.when(here)
    def _():
        arrive(xcol.at[pl.ds(0, group - 1)], r_x)

    @pl.when(jnp.logical_not(here))
    def _():
        arrive(xcol.at[pl.ds(0, group)], r_x)

    arrive(psib, r_p)
    mixed = (pbuf[core].astype(jnp.float32) + psib[...].astype(jnp.float32)).astype(jnp.bfloat16)
    held = xcol[pl.ds(core * group, group)].reshape(group * own, cols).astype(jnp.float32)
    res[me, core] = (held + mixed.astype(jnp.float32)).astype(jnp.bfloat16)
    for k in direct:
        push(res.at[me, core], res.at[me, core], s_res, r_res.at[me], flipped(me, k, ep), core)
    push(res.at[me, core], res.at[me, core], f_res, b_res.at[me], me, mate)
    for ref in (gacc, uacc, cgacc, cuacc, sq, gs):
        ref[...] = jnp.zeros_like(ref)
    arrive(wgu, wsem.at[2])
    arrive(cgu, wsem.at[3])

    def forward(e):
        push(res.at[e, core], res.at[e, core], f_res, b_res.at[e], me, mate)

    def absorb(e):
        arrive(res.at[e, mate], b_res.at[e])
        at = pl.ds(pl.multiple_of(e * cols, cols), cols)
        block = res[e].reshape(rows, cols).astype(jnp.float32)
        scaled = (block * gain2[:, at]).astype(jnp.bfloat16)
        gacc[...] += jnp.dot(scaled, wg[at, :], preferred_element_type=jnp.float32)
        uacc[...] += jnp.dot(scaled, wu[at, :], preferred_element_type=jnp.float32)
        cgacc[...] += across_dot(scaled, cg[:, at])
        cuacc[...] += across_dot(scaled, cu[:, at])
        wide_rows = scaled.astype(jnp.float32)
        for i in range(cols // 128):
            part_of = block[:, i * 128 : (i + 1) * 128]
            sq[...] += part_of * part_of
            line = cs[pl.ds(e * (cols // 128) + i, 1), :]
            gs[...] += wide_rows[:, i * 128 : (i + 1) * 128] * line

    ready = me
    for k in (1, 2, turn_at, *[k for k in range(3, ep) if k not in (turn_at, turned_by)], turned_by):
        e = flipped(me, k, ep)
        arrive(res.at[e, core], r_res.at[e])
        if k == turn_at:
            push(
                res.at[e, core], res.at[e, core], s_res, r_res.at[e],
                flipped(me, 1, ep), core,
            )
        forward(e)
        absorb(ready)
        ready = e
    absorb(ready)
    inv = lax.rsqrt(jnp.sum(sq[...], axis=-1, keepdims=True) / width + RMS_EPS)
    branch_scale = 1.0 / (1.0 + jnp.exp(-inv * jnp.sum(gs[...], axis=-1, keepdims=True)))
    expert = (me * tp + core) * wg.shape[1] // expert_cols
    table = share[...].astype(jnp.float32).reshape(rows, 128)
    picked = lax.broadcasted_iota(jnp.int32, (rows, 128), 1) == expert
    weight = jnp.sum(jnp.where(picked, table, 0.0), axis=-1, keepdims=True)

    def gated(target, gates, ups):
        g, u = gates[...] * inv, ups[...] * inv
        target[...] = (g / (1.0 + jnp.exp(-g)) * u).astype(jnp.bfloat16)

    gated(hid, gacc, uacc)
    gated(chid, cgacc, cuacc)
    arrive(wd, wsem.at[4])
    arrive(cd, wsem.at[5])
    pieces = mine.shape[0]
    piece = width // pieces
    last = own // tp

    def finish(n):
        arrive(sibin.at[n], r_sib.at[n])
        mine[n] = (
            sibout[n, core].astype(jnp.float32) + sibin[n].astype(jnp.float32)
        ).astype(jnp.bfloat16)
        for k in far:
            e = flipped(me, k, ep)
            push(mine.at[n, e], got.at[n, me], s_out, r_out.at[n], e, core)

    for n in range(pieces):
        at = slice(n * piece, (n + 1) * piece)
        y = weight * jnp.dot(hid[...], wd[:, at], preferred_element_type=jnp.float32)
        y = y + branch_scale * jnp.dot(chid[...], cd[:, at], preferred_element_type=jnp.float32)
        y = y.reshape(ep, tp, last, piece)
        for i in range(tp):
            sibout[n, i] = y[:, i].astype(jnp.bfloat16)
        push(sibout.at[n, mate], sibin.at[n], s_sib, r_sib.at[n], me, mate)
        if n:
            finish(n - 1)
    finish(pieces - 1)
    lax.fori_loop(own // 2, own, renew, 0)
    start = pl.multiple_of(lax.rem(me, group) * own, own)
    per = piece // cols
    for n in range(pieces):
        arrive(got.at[n, pl.ds(0, ep - 1)], r_out.at[n])
        total = mine[n, me].astype(jnp.float32)
        for k in far:
            total = total + got[n, flipped(me, k, ep)].astype(jnp.float32)
        for s in range(per):
            base = res[n * per + s, side, pl.ds(start, own)].astype(jnp.float32)
            base = jnp.where(core == 0, base[:last], base[last:])
            a = n * piece + s * cols
            out[:, a : a + cols] = (base + total[:, s * cols : (s + 1) * cols]).astype(jnp.bfloat16)
    arrive(rows_all.at[pl.ds(0, ep - 1)], s_row)
    arrive(part.at[pl.ds(0, ep - 1)], s_part)
    arrive(att_all.at[:, pl.ds(0, ep - 1)], s_att)
    arrive(share.at[pl.ds(0, ep - 1)], s_sh)
    arrive(psib, s_p)
    arrive(res.at[pl.ds(0, ep - 1), 0], s_res)
    arrive(res.at[:, 0], f_res)
    arrive(sibin, s_sib)
    arrive(got.at[:, pl.ds(0, ep - 1)], s_out)

    @pl.when(jnp.logical_not(here))
    def _():
        across.wait_send()

    @pl.when(here)
    def _():
        arrive(xcol.at[pl.ds(0, ep - 1)], s_x)


def settle_kernel(tokens, state, out, after, sems):
    step = state.shape[0] // (sems.shape[0] - 1)
    copies = [pltpu.make_async_copy(tokens, out, sems.at[0])]
    for i in range(sems.shape[0] - 1):
        at = pl.ds(i * step, step)
        copies.append(pltpu.make_async_copy(state.at[at], after.at[at], sems.at[i + 1]))
    for copy in copies:
        copy.start()
    for copy in copies:
        copy.wait()


def layer(*blocks):
    own = blocks[0].shape[0]
    cols, hidden = blocks[9].shape[1], blocks[18].shape[1]
    heads = blocks[17].shape[0]
    tiles = cols % 128 == 0 and hidden % 256 == 0 and own % 16 == 0
    tiles = tiles and heads % 8 == 0 and 128 % heads == 0 and heads <= 32
    tiles = tiles and blocks[0].shape[1] % 2048 == 0 and cols == 4 * LANE_WIDTH and own == 16
    ep = lax.axis_size("ep")
    heads_match = ep in (4, 8) and lax.axis_size("tp") == 2
    weights = sum(2 * w.size for w in blocks[18:24])
    rows = own * ep
    held = weights + rows * (12 * blocks[0].shape[1] + 8 * hidden) + 14 * blocks[1].size
    small = held < VMEM_ROOM
    return (kernel_body if tiles and heads_match and small else body)(*blocks)


def kernel_body(
    fresh_inputs,
    memory_arrays,
    chosen_specialist,
    chosen_coefficient,
    first_rescale,
    second_rescale,
    receiver_projector,
    address_projector,
    content_projector,
    final_projector,
    forget_narrowing,
    forget_widening,
    forget_bias,
    learning_narrowing,
    learning_widening,
    learning_bias,
    lane_scaling,
    instant_reward,
    specialist_switch,
    specialist_expand,
    specialist_contract,
    common_activator,
    common_expand,
    common_contract,
    common_switch,
):
    ep, tp = lax.axis_size("ep"), lax.axis_size("tp")
    own, width = fresh_inputs.shape
    half, cols = width // tp, final_projector.shape[1]
    heads = half // LANE_WIDTH
    group = ep // tp
    vmem = pl.BlockSpec(memory_space=pltpu.VMEM)
    hbm = pl.BlockSpec(memory_space=pl.ANY)
    bf16, f32 = jnp.bfloat16, jnp.float32
    dma = pltpu.SemaphoreType.DMA

    def row(vector):
        return vector.reshape(1, -1)

    rows, hidden, dense = ep * own, specialist_switch.shape[1], common_activator.shape[1]
    low, top = forget_narrowing.shape[1], chosen_specialist.shape[1]
    pack = 4
    wide, block_rows = pack * LANE_WIDTH, heads // pack * LANE_WIDTH
    pieces = 4
    piece, last = width // pieces, own // tp
    new_tokens, memory_after = pl.pallas_call(
        functools.partial(layer_kernel, ep, tp, FF_E),
        out_shape=(
            pltpu.VMEM((last, width), bf16),
            pltpu.VMEM(memory_arrays.shape, f32),
        ),
        in_specs=[hbm] * 25,
        out_specs=(vmem, vmem),
        scratch_shapes=[
            pltpu.VMEM((own, width), bf16),
            pltpu.VMEM((top, own), jnp.int32),
            pltpu.VMEM((top, own), bf16),
            pltpu.VMEM((2, 1, width), f32),
            pltpu.VMEM((width // 128, 128), bf16),
            pltpu.VMEM((width // 128, 128), f32),
            pltpu.VMEM((heads, LANE_WIDTH), f32),
            pltpu.VMEM((3, 1, half), f32),
            pltpu.VMEM((2, low, width), bf16),
            pltpu.VMEM((2, low, half), bf16),
            pltpu.VMEM((3, half, cols), bf16),
            pltpu.VMEM((half, cols), bf16),
            pltpu.VMEM((2, width, hidden), bf16),
            pltpu.VMEM((hidden, width), bf16),
            pltpu.VMEM((2, dense, width), bf16),
            pltpu.VMEM((dense, width), bf16),
            pltpu.VMEM((own, block_rows, wide), f32),
            pltpu.VMEM((own, block_rows, wide), bf16),
            pltpu.VMEM((tp, own, half), bf16),
            pltpu.VMEM((ep, own, half), bf16),
            pltpu.VMEM((ep, 3, own, cols), bf16),
            pltpu.VMEM((ep, 3, own, cols), bf16),
            pltpu.VMEM((own, half), f32),
            pltpu.VMEM((own, half), f32),
            pltpu.VMEM((1, half), f32),
            pltpu.VMEM((wide, wide), bf16),
            pltpu.VMEM((own, own, wide), bf16),
            pltpu.VMEM((heads // pack, 128, wide), bf16),
            pltpu.VMEM((heads // pack, LANE_WIDTH, 128), bf16),
            pltpu.VMEM((heads // pack, own, wide), bf16),
            pltpu.VMEM((heads // pack, ep, own, wide), bf16),
            pltpu.VMEM((ep, own, cols), bf16),
            pltpu.VMEM((ep, own, 128), bf16),
            pltpu.VMEM((tp, group * own, cols), bf16),
            pltpu.VMEM((group * own, cols), bf16),
            pltpu.VMEM((ep, tp, group * own, cols), bf16),
            pltpu.VMEM((rows, hidden), f32),
            pltpu.VMEM((rows, hidden), f32),
            pltpu.VMEM((rows, dense), f32),
            pltpu.VMEM((rows, dense), f32),
            pltpu.VMEM((rows, 128), f32),
            pltpu.VMEM((rows, 128), f32),
            pltpu.VMEM((rows, hidden), bf16),
            pltpu.VMEM((rows, dense), bf16),
            pltpu.VMEM((pieces, tp, ep, last, piece), bf16),
            pltpu.VMEM((pieces, ep, last, piece), bf16),
            pltpu.VMEM((pieces, ep, last, piece), bf16),
            pltpu.VMEM((pieces, ep, last, piece), bf16),
            dma((9,)),
            dma,
            dma((6,)),
            *[dma] * 5,
            dma((group,)),
            *[dma] * 2,
            dma((heads // pack,)),
            *[dma] * 7,
            dma((ep,)),
            dma,
            dma((ep,)),
            dma,
            dma((pieces,)),
            dma,
            dma((pieces,)),
        ],
        compiler_params=pltpu.CompilerParams(
            collective_id=0, has_side_effects=True, vmem_limit_bytes=54 * 2**20
        ),
        name="layer",
    )(
        fresh_inputs,
        memory_arrays,
        chosen_specialist.T,
        chosen_coefficient.T,
        row(first_rescale),
        row(second_rescale),
        common_switch.reshape(-1, 128),
        instant_reward,
        row(lane_scaling),
        receiver_projector,
        address_projector,
        content_projector,
        final_projector,
        forget_narrowing.T,
        forget_widening,
        row(forget_bias),
        learning_narrowing.T,
        learning_widening,
        row(learning_bias),
        specialist_switch,
        specialist_expand,
        specialist_contract,
        common_activator.T,
        common_expand.T,
        common_contract,
    )
    return pl.pallas_call(
        settle_kernel,
        out_shape=(
            jax.ShapeDtypeStruct((last, width), bf16),
            jax.ShapeDtypeStruct(memory_arrays.shape, f32),
        ),
        in_specs=[vmem] * 2,
        out_specs=(hbm,) * 2,
        scratch_shapes=[dma((5,))],
        compiler_params=pltpu.CompilerParams(vmem_limit_bytes=2**20),
        name="settle",
    )(
        pltpu.with_memory_space_constraint(new_tokens, pltpu.VMEM),
        pltpu.with_memory_space_constraint(memory_after, pltpu.VMEM),
    )


def solution(mesh):
    placed = (
        P(("grp", "ep"), None),
        P(("grp", "ep"), "tp", None, None),
        P(("grp", "ep"), None),
        P(("grp", "ep"), None),
        P(),
        P(),
        P("tp", "ep"),
        P("tp", "ep"),
        P("tp", "ep"),
        P("tp", "ep"),
        P(),
        P(None, "tp"),
        P("tp"),
        P(),
        P(None, "tp"),
        P("tp"),
        P("tp"),
        P("tp", None),
        P(None, ("ep", "tp")),
        P(None, ("ep", "tp")),
        P(("ep", "tp"), None),
        P(None, ("ep", "tp")),
        P(None, ("ep", "tp")),
        P(("ep", "tp"), None),
        P(),
    )
    return jax.shard_map(
        layer,
        mesh=mesh,
        in_specs=placed,
        out_specs=(P(("grp", "ep", "tp"), None), P(("grp", "ep"), "tp", None, None)),
        check_vma=False,
    )
```
